512 devices in a mesh: ep: 32 (over z, core), tp: 16 (over y, x).
Axes of the slice: x: 4, y: 4, z: 16, core: 2. Of those that a mesh axis runs over, the one named last changes fastest.
Arguments:
- resid: bfloat16 [256, 2048], P('ep', 'tp'), may hold values from -6 to 6
- attn_gain: float32 [2048], replicated, may hold values from 0.1 to 1.9
- w_query: bfloat16 [2048, 1024], P(None, 'tp'), may hold values from -0.125 to 0.125
- w_key: bfloat16 [2048, 1024], P(None, 'tp'), may hold values from -0.125 to 0.125
- w_value: bfloat16 [2048, 1024], P(None, 'tp'), may hold values from -0.125 to 0.125
- key_cache: bfloat16 [256, 16, 64, 1024], P('ep', 'tp'), may hold values from -6 to 6
- value_cache: bfloat16 [256, 16, 64, 1024], P('ep', 'tp'), may hold values from -19 to 19
- key_bias: float32 [256, 16, 1024], P('ep', 'tp'), may hold values from -10.2 to 0
- lengths: int32 [256], P('ep'), may hold values from 1 to 1024
- mix_gain: float32 [1024], P('tp'), may hold values from 0.1 to 1.9
- w_out: bfloat16 [1024, 2048], P('tp'), may hold values from -0.1875 to 0.1875
- ffn_gain: float32 [2048], replicated, may hold values from 0.1 to 1.9
- route_experts: int32 [256, 4], P('ep'), may hold values from 0 to 31, all different within a row; in each aligned block of 8 rows (0 to 7, 8 to 15, ...) at most 3 rows name the same one
- route_weights: float32 [256, 4], P('ep'), may hold values from 0.05 to 1
- w_gate: bfloat16 [32, 2048, 2048], P('ep', None, 'tp'), may hold values from -0.3125 to 0.3125
- w_up: bfloat16 [32, 2048, 2048], P('ep', None, 'tp'), may hold values from -0.3125 to 0.3125
- w_down: bfloat16 [32, 2048, 2048], P('ep', 'tp'), may hold values from -0.0546875 to 0.0546875
Outputs:
- mixed: bfloat16 [256, 2048], P('ep', 'tp')
- new_keys: bfloat16 [256, 1024], P('ep', 'tp')
- new_values: bfloat16 [256, 1024], P('ep', 'tp')
The draws below stay inside these ranges and needn't reach their ends.
Inputs may be any that keep to these rules, and one draw needn't show every extreme that they name: `route_experts`: each row names 4 different experts. Within the rows of one device (aligned blocks of 8 rows) no expert is named more than 3 times, a bound that some block reaches.
All inputs are finite; a program needn't handle non-finite values.
Results may differ from the reference program's by a relative error of at most 0.018.
Values may be sent and summed in bfloat16 or wider, within the bound.
No kernel may reach another device: no remote copies, remote signals or barrier semaphores. Data moves between devices by JAX's collectives and lax.ppermute only.
A program may use at most 64 MiB of HBM per device.

```python
import math
import jax
import jax.numpy as jnp
import numpy as np
from jax import lax

D = 2048
QUERY_GROUPS = 16
HEAD_DIM = 64
FF = 2048
TOP_K = 4
SEQS = 8
STORED_SLOTS = 1024
EXPERTS = 32
BATCH_STREAMS = 256
CAP = 3
SLICES = 16
N_EP = 32


def draw_value_cache(key, part):
    noise = jax.random.normal(jax.random.fold_in(key, 11), (BATCH_STREAMS, QUERY_GROUPS, HEAD_DIM, STORED_SLOTS), jnp.float32)
    center = 0.7 * jax.random.normal(jax.random.fold_in(key, 12), (BATCH_STREAMS, QUERY_GROUPS, HEAD_DIM, 1), jnp.float32)
    levels = 10.0 ** (0.5 * jnp.arange(QUERY_GROUPS, dtype=jnp.float32) / max(QUERY_GROUPS - 1, 1))
    values = jnp.clip(center + noise, -6.0, 6.0) * levels[None, :, None, None]
    return values.astype(jnp.bfloat16)


def draw_key_bias(key, part):
    slow_share = 0.5
    slow = jax.random.uniform(jax.random.fold_in(key, 21), (BATCH_STREAMS, QUERY_GROUPS), jnp.float32) < slow_share
    slow_base = jax.random.uniform(jax.random.fold_in(key, 22), (BATCH_STREAMS, QUERY_GROUPS), jnp.float32, -8.5, -7.0)
    fast_base = jax.random.uniform(jax.random.fold_in(key, 23), (BATCH_STREAMS, QUERY_GROUPS), jnp.float32, -3.5, -2.5)
    tilt = jax.random.uniform(jax.random.fold_in(key, 24), (BATCH_STREAMS, 1), jnp.float32, -0.7, 0.7)
    approximate_guess = jax.random.uniform(jax.random.fold_in(key, 25), (BATCH_STREAMS, QUERY_GROUPS, STORED_SLOTS), jnp.float32, -1.0, 1.0)
    spike_magnitude = jax.random.uniform(jax.random.fold_in(key, 26), (BATCH_STREAMS, QUERY_GROUPS, STORED_SLOTS), jnp.float32) < 3.0 / STORED_SLOTS
    raised_entries = jax.random.uniform(jax.random.fold_in(key, 27), (BATCH_STREAMS, QUERY_GROUPS, STORED_SLOTS), jnp.float32, -1.5, 0.0)
    floor_offset = jnp.where(slow, slow_base, fast_base) + tilt
    return jnp.where(spike_magnitude, raised_entries, floor_offset[:, :, None] + approximate_guess).astype(jnp.float32)


def place_ends(array, rng, least, top_value):
    extent = array.shape
    place = [jax.random.randint(jax.random.fold_in(rng, axis), (), 0, extent[axis]) for axis in range(len(extent))]
    array = array.at[tuple(place)].set(least)
    longest = extent.index(max(extent))
    place[longest] = (place[longest] + 1) % extent[longest]
    return array.at[tuple(place)].set(top_value)


def level_of(key, shape, cuts, least, top_value):
    def one(dim, shards_of):
        steps = jax.random.uniform(jax.random.fold_in(jax.random.fold_in(key, 6), dim), (shards_of,), jnp.float32, least / len(cuts), top_value / len(cuts))
        return jnp.repeat(jnp.exp(steps), shape[dim] // shards_of).reshape((-1,) + (1,) * (len(shape) - dim - 1))

    factor_of = one(*cuts[0])
    for cut in cuts[1:]:
        factor_of = factor_of * one(*cut)
    return factor_of


def shared_out(stream_key, own, number, rows, amount, top, most, lean):
    sequence = jax.random.permutation(stream_key, amount)
    crowded, common = load_shares(amount, rows * top, most, lean, True), load_shares(amount, rows * top, most, lean, False)
    places = jnp.arange(amount)

    def named(sizes, offset_by):
        used = int((sizes > 0).sum())
        fixed = max(1, used // 4)
        shifted = fixed + (places - fixed + offset_by * (used - fixed)) % max(1, amount - fixed)
        return jnp.zeros((amount,), jnp.int32).at[sequence[jnp.where(places < fixed, places, shifted)]].set(jnp.asarray(sizes, jnp.int32))

    sizes = jnp.where(number % 4 == 0, named(crowded, number // 4), named(common, number - number // 4 - 1))
    mixed = jax.random.permutation(jax.random.fold_in(own, 3), amount)
    donor, taker = mixed[0:amount // 2 * 2:2], mixed[1:amount // 2 * 2:2]
    room = jnp.minimum(sizes[donor] - 1, most - sizes[taker]) // 2
    room = jnp.where((donor == sequence[0]) | (taker == sequence[0]) | (sizes[taker] == 0), 0, jnp.maximum(room, 0))
    shifted = jax.random.randint(jax.random.fold_in(own, 4), (amount // 2,), 0, 1 << 20) % (room + 1)
    sizes = sizes.at[donor].add(-shifted).at[taker].add(shifted)
    labels = jnp.searchsorted(jnp.cumsum(sizes), jnp.arange(rows * top), side="right").astype(jnp.int32)
    listing = labels.reshape(top, rows).T
    listing = listing[jax.random.permutation(jax.random.fold_in(own, 1), rows)]
    offset_by = jax.random.randint(jax.random.fold_in(own, 2), (rows, 1), 0, top)
    return jnp.take_along_axis(listing, (jnp.arange(top)[None, :] + offset_by) % top, axis=1)


def load_shares(number_of, total, bound, slope, full):
    portions = [(1 << 20) // math.isqrt(grade ** slope) + 1 for grade in range(1, number_of + 1)]
    largest = bound if full else min(bound, max(-(-total // number_of), total * portions[0] // sum(portions)))
    least = 1 if total - largest >= number_of - 1 else 0
    given, spare = [largest] + [least] * (number_of - 1), total - largest - least * (number_of - 1)
    while spare > 0:
        movable = [i for i in range(1, number_of) if given[i] < largest] or [i for i in range(1, number_of) if given[i] < bound]
        mass, budget = sum([portions[i] for i in movable]), spare
        for i in movable:
            more = min(bound - given[i], max(1, budget * portions[i] // mass), spare)
            given[i] = given[i] + more
            spare = spare - more
    return np.array(given)


def scatter_about(rng, shape, scale, most, shards=(), kind=jnp.bfloat16):
    level = level_of(rng, shape, shards, -0.22, 0.18) if shards else 1.0
    entries = jax.random.normal(rng, shape, jnp.float32) * scale * level
    return jnp.minimum(jnp.maximum(entries, -most), most).astype(kind)


def setup_inputs(seed: int = 0) -> dict:
    seeds = jax.random.split(jax.random.key(seed), 18)
    resid = scatter_about(seeds[0], (BATCH_STREAMS, D), 1.0, 6.0, ((0, 32), (1, 16)))
    attn_gain = jnp.clip(1.0 + 0.18 * jax.random.normal(seeds[1], (D,), jnp.float32), 0.1, 1.9)
    w_query = scatter_about(seeds[2], (D, QUERY_GROUPS * HEAD_DIM), D ** -0.5, 0.125, ((1, 16),))
    w_key = scatter_about(seeds[3], (D, QUERY_GROUPS * HEAD_DIM), D ** -0.5, 0.125, ((1, 16),))
    w_value = scatter_about(seeds[4], (D, QUERY_GROUPS * HEAD_DIM), D ** -0.5, 0.125, ((1, 16),))
    key_cache = scatter_about(seeds[5], (BATCH_STREAMS, QUERY_GROUPS, HEAD_DIM, STORED_SLOTS), 1.0, 6.0, ((0, 32), (1, 16)))
    value_cache = draw_value_cache(jax.random.fold_in(seeds[17], 71), 0)
    key_bias = draw_key_bias(jax.random.fold_in(seeds[17], 71), 0)
    lengths = place_ends(jax.random.randint(seeds[8], (BATCH_STREAMS,), 1, STORED_SLOTS + 1), jax.random.fold_in(seeds[8], 1), 1, STORED_SLOTS).astype(jnp.int32)
    mix_gain = jnp.clip(1.0 + 0.18 * jax.random.normal(seeds[9], (QUERY_GROUPS * HEAD_DIM,), jnp.float32), 0.1, 1.9)
    w_out = scatter_about(seeds[10], (QUERY_GROUPS * HEAD_DIM, D), (QUERY_GROUPS * HEAD_DIM) ** -0.5, 0.1875, ((0, 16),))
    ffn_gain = jnp.clip(1.0 + 0.18 * jax.random.normal(seeds[11], (D,), jnp.float32), 0.1, 1.9)
    route_experts_keys = jax.random.split(jax.random.fold_in(seeds[12], 1), BATCH_STREAMS // SEQS)
    route_experts_turns = jax.random.permutation(jax.random.fold_in(seeds[12], 3), BATCH_STREAMS // SEQS)
    route_experts = jax.vmap(lambda own, number: shared_out(jax.random.fold_in(seeds[12], 2), own, number, SEQS, EXPERTS, TOP_K, CAP, 2))(route_experts_keys, route_experts_turns).reshape((BATCH_STREAMS, TOP_K))
    route_weights = jnp.clip(jnp.exp(math.log(1.0) - 2.9957323 * jax.random.uniform(seeds[13], (BATCH_STREAMS, TOP_K), jnp.float32) ** level_of(seeds[13], (BATCH_STREAMS, TOP_K), ((0, 32),), -0.2, 0.2)), 0.05, 1.0)
    w_gate = scatter_about(seeds[14], (EXPERTS, D, FF), (2.5 / D ** 0.5), 0.3125, ((0, 32), (2, 16)))
    w_up = scatter_about(seeds[15], (EXPERTS, D, FF), (2.5 / D ** 0.5), 0.3125, ((0, 32), (2, 16)))
    w_down = scatter_about(seeds[16], (EXPERTS, FF, D), (0.4 / FF ** 0.5), 0.0546875, ((0, 32), (1, 16)))
    return {"resid": resid, "attn_gain": attn_gain, "w_query": w_query, "w_key": w_key, "w_value": w_value, "key_cache": key_cache, "value_cache": value_cache, "key_bias": key_bias, "lengths": lengths, "mix_gain": mix_gain, "w_out": w_out, "ffn_gain": ffn_gain, "route_experts": route_experts, "route_weights": route_weights, "w_gate": w_gate, "w_up": w_up, "w_down": w_down}


eps = 1e-06
limit = 7.0
alpha = 1.702

def rms_rows(values, gain):
    return values * lax.rsqrt(lax.optimization_barrier(jnp.mean(values * values, axis=-1, keepdims=True)) + eps) * gain

def stick_one(query, keys, values, bias, length):
    scores = jnp.einsum('hd,hds->hs', query.astype(jnp.float32), keys.astype(jnp.float32)) * HEAD_DIM ** (-0.5) + bias
    live = jnp.arange(STORED_SLOTS, dtype=jnp.int32)[None, :] < length
    log_keep = jnp.where(live, jax.nn.log_sigmoid(-scores), 0.0)
    after = lax.cumsum(log_keep, axis=1, reverse=True) - log_keep
    weights = jnp.where(live, jnp.exp(jax.nn.log_sigmoid(scores) + after), 0.0).astype(jnp.bfloat16)
    return jnp.einsum('hs,hds->hd', weights.astype(jnp.float32), values.astype(jnp.float32))

def reference(resid, attn_gain, w_query, w_key, w_value, key_cache, value_cache, key_bias, lengths, mix_gain, w_out, ffn_gain, route_experts, route_weights, w_gate, w_up, w_down):
    whole = resid.astype(jnp.float32)
    normed_in = rms_rows(whole, attn_gain).astype(jnp.bfloat16)
    query = jnp.dot(normed_in, w_query, preferred_element_type=jnp.float32).astype(jnp.bfloat16)
    new_keys = jnp.dot(normed_in, w_key, preferred_element_type=jnp.float32).astype(jnp.bfloat16)
    new_values = jnp.dot(normed_in, w_value, preferred_element_type=jnp.float32).astype(jnp.bfloat16)
    head_query = query.reshape(BATCH_STREAMS, QUERY_GROUPS, HEAD_DIM)

    def attend(item):
        return stick_one(item[0], item[1], item[2], item[3], item[4])
    attended = lax.map(attend, (head_query, key_cache, value_cache, key_bias, lengths)).reshape(BATCH_STREAMS, QUERY_GROUPS * HEAD_DIM)
    normed_heads = rms_rows(attended, mix_gain).astype(jnp.bfloat16)
    block = QUERY_GROUPS * HEAD_DIM // SLICES
    partial_heads = jnp.einsum('njr,jrd->njd', normed_heads.reshape(BATCH_STREAMS, SLICES, block).astype(jnp.float32), w_out.reshape(SLICES, block, D).astype(jnp.float32))
    partial_heads = lax.optimization_barrier(partial_heads.astype(jnp.bfloat16)).astype(jnp.float32)
    middle = whole + lax.optimization_barrier(jnp.sum(partial_heads, axis=1))
    normed_mid = rms_rows(middle, ffn_gain).astype(jnp.bfloat16)
    share = route_weights / lax.optimization_barrier(jnp.sum(route_weights, axis=1, keepdims=True))
    chosen = route_experts.reshape(N_EP, SEQS * TOP_K)
    position = jnp.arange(SEQS * TOP_K, dtype=jnp.int32)
    earlier = (chosen[:, :, None] == chosen[:, None, :]) & (position[:, None] > position[None, :])[None]
    rank = lax.optimization_barrier(jnp.sum(earlier.astype(jnp.int32), axis=2))
    slot = (jnp.arange(N_EP, dtype=jnp.int32)[:, None] * CAP + rank).reshape(-1)
    expert_flat = route_experts.reshape(-1)
    token_flat = jnp.repeat(jnp.arange(BATCH_STREAMS, dtype=jnp.int32), TOP_K)
    table = jnp.zeros((EXPERTS, N_EP * CAP), jnp.int32).at[expert_flat, slot].set(token_flat)
    hidden_block = FF // SLICES

    def one_expert(item):
        gate_weight, up_weight, down_weight, row_index = item
        inputs = normed_mid[row_index]
        gate = jnp.minimum(jnp.dot(inputs, gate_weight, preferred_element_type=jnp.float32), limit)
        upper = jnp.clip(jnp.dot(inputs, up_weight, preferred_element_type=jnp.float32), -limit, limit)
        active = ((upper + 1.0) * gate * jax.nn.sigmoid(alpha * gate)).astype(jnp.bfloat16)
        pieces = jnp.einsum('sjf,jfd->sjd', active.reshape(-1, SLICES, hidden_block).astype(jnp.float32), down_weight.reshape(SLICES, hidden_block, D).astype(jnp.float32))
        pieces = lax.optimization_barrier(pieces.astype(jnp.bfloat16)).astype(jnp.float32)
        return lax.optimization_barrier(jnp.sum(pieces, axis=1)).astype(jnp.bfloat16)
    outputs = lax.map(one_expert, (w_gate, w_up, w_down, table))
    picked = outputs[expert_flat, slot].astype(jnp.float32).reshape(BATCH_STREAMS, TOP_K, D)
    mixture = lax.optimization_barrier(jnp.sum(share[:, :, None] * picked, axis=1))
    mixed = (middle + mixture).astype(jnp.bfloat16)
    return (mixed, new_keys, new_values)
```

```python
import jax
import jax.numpy as jnp
from jax import lax
from jax.experimental import pallas as pl
from jax.experimental.pallas import tpu as pltpu
from jax.sharding import Mesh
from jax.sharding import PartitionSpec as P

TP = ("tp_0", "tp_1")

eps = 1e-06
limit = 7.0
alpha = 1.702
LANES = 128
SLOTS = 4
CAP = 3


def from_everyone(x, axis):
    size = lax.axis_size(axis)
    return lax.all_to_all(jnp.broadcast_to(x[None], (size, *x.shape)), axis, 0, 0, tiled=True)


def attend_kernel(lengths_ref, parts_ref, gain_ref, wq_ref, key_ref, value_ref, bias_ref,
                  mix_ref, wout_ref, normed_ref, out_ref):
    blocks, rows, lanes = parts_ref.shape
    heads = key_ref.shape[2]
    cache = key_ref.shape[3]
    xs = [parts_ref[t].astype(jnp.float32) for t in range(blocks)]
    total = xs[0] * xs[0]
    for x in xs[1:]:
        total = total + x * x
    width = blocks * lanes
    scale = lax.rsqrt(jnp.sum(total, axis=1, keepdims=True) / width + eps)
    normed = jnp.concatenate(
        [(xs[t] * scale * gain_ref[t : t + 1, :]).astype(jnp.bfloat16) for t in range(blocks)],
        axis=1,
    )
    normed_ref[...] = normed
    query = jnp.dot(normed, wq_ref[...], preferred_element_type=jnp.float32).astype(jnp.bfloat16)
    query = query.astype(jnp.float32)
    spread = jnp.concatenate([query] * rows, axis=1)
    row = lax.broadcasted_iota(jnp.int32, spread.shape, 0)
    own = lax.broadcasted_iota(jnp.int32, spread.shape, 1) // heads == row
    spread = jnp.where(own, spread, 0.0).astype(jnp.bfloat16)
    keys = key_ref[:, 0].reshape(rows * heads, cache)
    scores = jnp.dot(spread, keys, preferred_element_type=jnp.float32) * heads ** (-0.5)
    scores = scores + bias_ref[:, 0, :]
    line = lax.broadcasted_iota(jnp.int32, (rows, cache), 0)
    length = jnp.zeros((rows, cache), jnp.int32)
    for n in range(rows):
        length = jnp.where(line == n, lengths_ref[n], length)
    live = lax.broadcasted_iota(jnp.int32, (rows, cache), 1) < length
    soft = jnp.maximum(scores, 0.0) + jnp.log1p(jnp.exp(-jnp.abs(scores)))
    drop = jnp.where(live, soft, 0.0)
    chunks = cache // lanes
    stacked = jnp.concatenate([drop[:, c * lanes : (c + 1) * lanes] for c in range(chunks)], axis=0)
    below = lax.broadcasted_iota(jnp.int32, (lanes, lanes), 0)
    across = lax.broadcasted_iota(jnp.int32, (lanes, lanes), 1)
    later = (below > across).astype(jnp.bfloat16)
    high = stacked.astype(jnp.bfloat16)
    rest = stacked - high.astype(jnp.float32)
    middle = rest.astype(jnp.bfloat16)
    low = (rest - middle.astype(jnp.float32)).astype(jnp.bfloat16)
    after = (
        jnp.dot(high, later, preferred_element_type=jnp.float32)
        + jnp.dot(middle, later, preferred_element_type=jnp.float32)
        + jnp.dot(low, later, preferred_element_type=jnp.float32)
    )
    sums = jnp.sum(stacked, axis=1, keepdims=True)
    running = jnp.zeros((rows, 1), jnp.float32)
    pieces = [None] * chunks
    for c in reversed(range(chunks)):
        pieces[c] = after[c * rows : (c + 1) * rows] + running
        running = running + sums[c * rows : (c + 1) * rows]
    after = jnp.concatenate(pieces, axis=1)
    weights = jnp.where(live, jnp.exp(scores - soft - after), 0.0).astype(jnp.bfloat16)
    values = value_ref[:, 0].reshape(rows * heads, cache)
    crossed = lax.dot_general(
        weights, values, (((1,), (1,)), ((), ())), preferred_element_type=jnp.float32
    )
    crossed = jnp.where(own, crossed, 0.0)
    folded = crossed[:, :lanes]
    for c in range(1, crossed.shape[1] // lanes):
        folded = folded + crossed[:, c * lanes : (c + 1) * lanes]
    square = jnp.sum(folded * folded, axis=1, keepdims=True)
    attended = folded[:, :heads] + folded[:, heads : 2 * heads]
    ready = (attended * mix_ref[...]).astype(jnp.bfloat16)
    branch = jnp.dot(ready, wout_ref[...], preferred_element_type=jnp.float32)
    top = square.astype(jnp.bfloat16).astype(jnp.float32)
    half = lax.broadcasted_iota(jnp.int32, (rows, lanes), 1) < lanes // 2
    tail = jnp.where(half, top, square - top)
    for t in range(blocks):
        both = jnp.concatenate([branch[:, t * lanes : (t + 1) * lanes], tail], axis=0)
        out_ref[t] = both.astype(jnp.bfloat16)


def expert_kernel(rows_ref, gain_ref, gate_ref, up_ref, down_ref, out_ref):
    blocks, rows, lanes = rows_ref.shape
    total = jnp.zeros((rows, lanes), jnp.float32)
    scaled = []
    for t in range(blocks):
        x = rows_ref[t].astype(jnp.float32)
        total = total + x * x
        scaled.append((x * gain_ref[t : t + 1, :]).astype(jnp.bfloat16))
    scaled = jnp.concatenate(scaled, axis=1)
    scale = lax.rsqrt(jnp.sum(total, axis=1, keepdims=True) / (blocks * lanes) + eps)
    gate = jnp.dot(scaled, gate_ref[0], preferred_element_type=jnp.float32) * scale
    upper = jnp.dot(scaled, up_ref[0], preferred_element_type=jnp.float32) * scale
    gate = jnp.minimum(gate, limit)
    upper = jnp.clip(upper, -limit, limit)
    active = ((upper + 1.0) * gate * jax.nn.sigmoid(alpha * gate)).astype(jnp.bfloat16)
    result = jnp.dot(active, down_ref[0], preferred_element_type=jnp.float32).astype(jnp.bfloat16)
    for t in range(blocks):
        out_ref[t] = result[:, t * lanes : (t + 1) * lanes]


def vmem():
    return pl.BlockSpec(memory_space=pltpu.VMEM)


def body(
    resid,
    attn_gain,
    w_query,
    w_key,
    w_value,
    key_cache,
    value_cache,
    key_bias,
    lengths,
    mix_gain,
    w_out,
    ffn_gain,
    route_experts,
    route_weights,
    w_gate,
    w_up,
    w_down,
):
    blocks = lax.axis_size(TP)
    rows, lanes = resid.shape
    width = blocks * lanes
    parts = from_everyone(resid, TP)
    normed_in, partial_branch = pl.pallas_call(
        attend_kernel,
        in_specs=[pl.BlockSpec(memory_space=pltpu.SMEM)] + [vmem()] * 8,
        out_specs=[vmem(), vmem()],
        out_shape=[
            jax.ShapeDtypeStruct((rows, width), jnp.bfloat16),
            jax.ShapeDtypeStruct((blocks, 2 * rows, lanes), jnp.bfloat16),
        ],
        name="attend",
    )(
        lengths,
        parts,
        attn_gain.reshape(blocks, lanes),
        w_query,
        key_cache,
        value_cache,
        key_bias,
        mix_gain.reshape(1, -1),
        w_out,
    )
    new_keys = jnp.dot(normed_in, w_key, preferred_element_type=jnp.float32).astype(jnp.bfloat16)
    new_values = jnp.dot(normed_in, w_value, preferred_element_type=jnp.float32).astype(
        jnp.bfloat16
    )
    summed = jnp.sum(
        lax.all_to_all(partial_branch, TP, 0, 0, tiled=True).astype(jnp.float32), axis=0
    )
    channels = mix_gain.shape[0] * blocks
    square = summed[rows:, :1] + summed[rows:, lanes - 1 :]
    middle = resid.astype(jnp.float32) + summed[:rows] * lax.rsqrt(square / channels + eps)

    top = route_experts.shape[1]
    share = route_weights / jnp.sum(route_weights, axis=1, keepdims=True)
    groups = lax.axis_size("ep")
    experts_all = w_gate.shape[0] * groups
    count = rows * top
    position = lax.broadcasted_iota(jnp.int32, (count, count), 0)
    later = position > position.T
    chosen = route_experts.reshape(-1)
    earlier = (chosen[:, None] == chosen[None, :]) & later
    rank = jnp.sum(earlier.astype(jnp.int32), axis=1)
    target = chosen * SLOTS + rank
    slots_total = experts_all * SLOTS
    slot_iota = lax.broadcasted_iota(jnp.int32, (slots_total, rows, top), 0)
    dispatch = jnp.any(slot_iota == target.reshape(rows, top)[None], axis=2).astype(jnp.bfloat16)
    outgoing = jnp.dot(
        dispatch, middle.astype(jnp.bfloat16), preferred_element_type=jnp.float32
    ).astype(jnp.bfloat16)
    arrived = lax.all_to_all(
        outgoing.reshape(experts_all, SLOTS, lanes), "ep", split_axis=0, concat_axis=0, tiled=True
    )
    items = groups * CAP
    item = lax.broadcasted_iota(jnp.int32, (items, slots_total), 0)
    slot = lax.broadcasted_iota(jnp.int32, (items, slots_total), 1)
    packed = (item // CAP * SLOTS + item % CAP == slot).astype(jnp.bfloat16)
    held = jnp.dot(
        packed, arrived.reshape(slots_total, lanes), preferred_element_type=jnp.float32
    ).astype(jnp.bfloat16)
    gathered = from_everyone(held, TP)
    partial_out = pl.pallas_call(
        expert_kernel,
        in_specs=[vmem()] * 5,
        out_specs=vmem(),
        out_shape=jax.ShapeDtypeStruct((blocks, items, lanes), jnp.bfloat16),
        name="expert",
    )(gathered, ffn_gain.reshape(blocks, lanes), w_gate, w_up, w_down)
    result = jnp.sum(
        lax.all_to_all(partial_out, TP, 0, 0, tiled=True).astype(jnp.float32), axis=0
    ).astype(jnp.bfloat16)
    spaced = jnp.dot(packed.T, result, preferred_element_type=jnp.float32).astype(jnp.bfloat16)
    returned = lax.all_to_all(
        spaced.reshape(groups, SLOTS, lanes), "ep", split_axis=0, concat_axis=0, tiled=True
    )
    picker = (target[:, None] == lax.broadcasted_iota(jnp.int32, (count, slots_total), 1)).astype(
        jnp.bfloat16
    )
    picked = jnp.dot(
        picker, returned.reshape(slots_total, lanes), preferred_element_type=jnp.float32
    ).reshape(rows, top, lanes)
    mixture = jnp.sum(share[:, :, None] * picked, axis=1)
    mixed = (middle + mixture).astype(jnp.bfloat16)
    return (mixed, new_keys, new_values)


def solution(mesh):
    torus = Mesh(mesh.devices.reshape(mesh.shape["ep"], 4, 4), ("ep", "tp_0", "tp_1"))
    in_specs = (
        P("ep", TP),
        P(),
        P(None, TP),
        P(None, TP),
        P(None, TP),
        P("ep", TP, None, None),
        P("ep", TP, None, None),
        P("ep", TP, None),
        P("ep"),
        P(TP),
        P(TP, None),
        P(),
        P("ep", None),
        P("ep", None),
        P("ep", None, TP),
        P("ep", None, TP),
        P("ep", TP, None),
    )
    out_specs = (P("ep", TP), P("ep", TP), P("ep", TP))
    return jax.shard_map(body, mesh=torus, in_specs=in_specs, out_specs=out_specs, check_vma=False)
```

```python
import jax
import jax.numpy as jnp
from jax import lax
from jax.experimental import pallas as pl
from jax.experimental.pallas import tpu as pltpu
from jax.sharding import Mesh
from jax.sharding import PartitionSpec as P

TP = ("tp_0", "tp_1")

eps = 1e-06
limit = 7.0
alpha = 1.702
LANES = 128
SLOTS = 4
CAP = 3
LIMIT = 16 * 1024 * 1024
LONG = 4 * 10**10
SHORT = 10**9


def project(rows, weight_ref):
    return lax.dot_general(
        rows, weight_ref[...], (((1,), (1,)), ((), ())), preferred_element_type=jnp.float32
    ).astype(jnp.bfloat16)


def attend_kernel(lengths_ref, parts_ref, gain_ref, wq_ref, wk_ref, wv_ref, key_ref, value_ref,
                  bias_ref, mix_ref, wout_ref, new_key_ref, new_value_ref, out_ref):
    blocks, rows, lanes = parts_ref.shape
    heads = key_ref.shape[2]
    cache = key_ref.shape[3]
    xs = [parts_ref[t].astype(jnp.float32) for t in range(blocks)]
    total = xs[0] * xs[0]
    for x in xs[1:]:
        total = total + x * x
    width = blocks * lanes
    scale = lax.rsqrt(jnp.sum(total, axis=1, keepdims=True) / width + eps)
    normed = jnp.concatenate(
        [(xs[t] * scale * gain_ref[t : t + 1, :]).astype(jnp.bfloat16) for t in range(blocks)],
        axis=1,
    )
    query = project(normed, wq_ref).astype(jnp.float32)
    spread = jnp.concatenate([query] * rows, axis=1)
    row = lax.broadcasted_iota(jnp.int32, spread.shape, 0)
    own = lax.broadcasted_iota(jnp.int32, spread.shape, 1) // heads == row
    spread = jnp.where(own, spread, 0.0).astype(jnp.bfloat16)
    keys = key_ref[:, 0].reshape(rows * heads, cache)
    scores = jnp.dot(spread, keys, preferred_element_type=jnp.float32) * heads ** (-0.5)
    scores = scores + bias_ref[:, 0, :]
    line = lax.broadcasted_iota(jnp.int32, (rows, cache), 0)
    length = jnp.zeros((rows, cache), jnp.int32)
    for n in range(rows):
        length = jnp.where(line == n, lengths_ref[n], length)
    live = lax.broadcasted_iota(jnp.int32, (rows, cache), 1) < length
    soft = jnp.maximum(scores, 0.0) + jnp.log1p(jnp.exp(-jnp.abs(scores)))
    drop = jnp.where(live, soft, 0.0)
    chunks = cache // lanes
    stacked = jnp.concatenate([drop[:, c * lanes : (c + 1) * lanes] for c in range(chunks)], axis=0)
    below = lax.broadcasted_iota(jnp.int32, (lanes, lanes), 0)
    across = lax.broadcasted_iota(jnp.int32, (lanes, lanes), 1)
    later = (below > across).astype(jnp.bfloat16)
    high = stacked.astype(jnp.bfloat16)
    rest = stacked - high.astype(jnp.float32)
    middle = rest.astype(jnp.bfloat16)
    low = (rest - middle.astype(jnp.float32)).astype(jnp.bfloat16)
    after = (
        jnp.dot(high, later, preferred_element_type=jnp.float32)
        + jnp.dot(middle, later, preferred_element_type=jnp.float32)
        + jnp.dot(low, later, preferred_element_type=jnp.float32)
    )
    sums = jnp.sum(stacked, axis=1, keepdims=True)
    running = jnp.zeros((rows, 1), jnp.float32)
    pieces = [None] * chunks
    for c in reversed(range(chunks)):
        pieces[c] = after[c * rows : (c + 1) * rows] + running
        running = running + sums[c * rows : (c + 1) * rows]
    after = jnp.concatenate(pieces, axis=1)
    weights = jnp.where(live, jnp.exp(scores - soft - after), 0.0).astype(jnp.bfloat16)
    values = value_ref[:, 0].reshape(rows * heads, cache)
    crossed = lax.dot_general(
        weights, values, (((1,), (1,)), ((), ())), preferred_element_type=jnp.float32
    )
    crossed = jnp.where(own, crossed, 0.0)
    folded = crossed[:, :lanes]
    for c in range(1, crossed.shape[1] // lanes):
        folded = folded + crossed[:, c * lanes : (c + 1) * lanes]
    square = jnp.sum(folded * folded, axis=1, keepdims=True)
    attended = folded[:, :heads] + folded[:, heads : 2 * heads]
    ready = (attended * mix_ref[...]).astype(jnp.bfloat16)
    branch = jnp.dot(ready, wout_ref[...], preferred_element_type=jnp.float32)
    top = square.astype(jnp.bfloat16).astype(jnp.float32)
    half = lax.broadcasted_iota(jnp.int32, (rows, lanes), 1) < lanes // 2
    tail = jnp.where(half, top, square - top)
    for t in range(blocks):
        both = jnp.concatenate([branch[:, t * lanes : (t + 1) * lanes], tail], axis=0)
        out_ref[t] = both.astype(jnp.bfloat16)
    new_key_ref[...] = project(normed, wk_ref)
    new_value_ref[...] = project(normed, wv_ref)


def chosen_slots(experts_ref, slots):
    top, rows = experts_ref.shape
    slot = lax.broadcasted_iota(jnp.int32, (slots, rows), 0)
    hits = [experts_ref[k : k + 1, :] == slot // SLOTS for k in range(top)]
    named = hits[0]
    for hit in hits[1:]:
        named = named | hit
    first = lax.broadcasted_iota(jnp.int32, (rows, rows), 0)
    second = lax.broadcasted_iota(jnp.int32, (rows, rows), 1)
    earlier = (first < second).astype(jnp.bfloat16)
    rank = jnp.dot(
        named.astype(jnp.bfloat16), earlier, preferred_element_type=jnp.float32
    ).astype(jnp.int32)
    return hits, named & (rank == slot % SLOTS)


def copies_kernel(row_ref, out_ref):
    for t in range(out_ref.shape[0]):
        out_ref[t] = row_ref[...]


def middle_kernel(parts_ref, resid_ref, experts_ref, middle_ref, out_ref):
    blocks, both, lanes = parts_ref.shape
    rows = both // 2
    total = parts_ref[0].astype(jnp.float32)
    for t in range(1, blocks):
        total = total + parts_ref[t].astype(jnp.float32)
    square = total[rows:, :1] + total[rows:, lanes - 1 :]
    channels = blocks * (lanes // 2)
    scale = lax.rsqrt(square / channels + eps)
    middle = resid_ref[...].astype(jnp.float32) + total[:rows] * scale
    middle_ref[...] = middle
    groups, slots, _ = out_ref.shape
    _, placed = chosen_slots(experts_ref, groups * slots)
    out = jnp.dot(
        placed.astype(jnp.bfloat16),
        middle.astype(jnp.bfloat16),
        preferred_element_type=jnp.float32,
    )
    out_ref[...] = out.reshape(groups, slots, lanes).astype(jnp.bfloat16)


def packing(items, slots):
    item = lax.broadcasted_iota(jnp.int32, (items, slots), 0)
    slot = lax.broadcasted_iota(jnp.int32, (items, slots), 1)
    return (item // CAP * SLOTS + item % CAP == slot).astype(jnp.bfloat16)


def spread_kernel(arrived_ref, out_ref):
    blocks, items, lanes = out_ref.shape
    groups, slots, _ = arrived_ref.shape
    arrived = arrived_ref[...].astype(jnp.float32).reshape(groups * slots, lanes)
    held = jnp.dot(
        packing(items, groups * slots),
        arrived.astype(jnp.bfloat16),
        preferred_element_type=jnp.float32,
    ).astype(jnp.bfloat16)
    for t in range(blocks):
        out_ref[t] = held


def total_kernel(parts_ref, out_ref):
    blocks, items, lanes = parts_ref.shape
    groups, slots, _ = out_ref.shape
    total = parts_ref[0].astype(jnp.float32)
    for t in range(1, blocks):
        total = total + parts_ref[t].astype(jnp.float32)
    spaced = lax.dot_general(
        packing(items, groups * slots),
        total.astype(jnp.bfloat16),
        (((0,), (0,)), ((), ())),
        preferred_element_type=jnp.float32,
    )
    out_ref[...] = spaced.reshape(groups, slots, lanes).astype(jnp.bfloat16)


def mixture_kernel(returned_ref, middle_ref, experts_ref, share_ref, out_ref):
    groups, slots, lanes = returned_ref.shape
    hits, placed = chosen_slots(experts_ref, groups * slots)
    share = share_ref[...]
    share = share / jnp.sum(share, axis=0, keepdims=True)
    weight = jnp.where(hits[0], share[:1, :], 0.0)
    for k in range(1, len(hits)):
        weight = weight + jnp.where(hits[k], share[k : k + 1, :], 0.0)
    weight = jnp.where(placed, weight, 0.0)
    high = weight.astype(jnp.bfloat16)
    low = (weight - high.astype(jnp.float32)).astype(jnp.bfloat16)
    returned = returned_ref[...].astype(jnp.float32).reshape(groups * slots, lanes)
    returned = returned.astype(jnp.bfloat16)
    mixture = sum(
        lax.dot_general(
            part, returned, (((0,), (0,)), ((), ())), preferred_element_type=jnp.float32
        )
        for part in (high, low)
    )
    out_ref[...] = (middle_ref[...] + mixture).astype(jnp.bfloat16)


def expert_kernel(rows_ref, gain_ref, gate_ref, up_ref, down_ref, out_ref):
    blocks, rows, lanes = rows_ref.shape
    total = jnp.zeros((rows, lanes), jnp.float32)
    scaled = []
    for t in range(blocks):
        x = rows_ref[t].astype(jnp.float32)
        total = total + x * x
        scaled.append((x * gain_ref[t : t + 1, :]).astype(jnp.bfloat16))
    scaled = jnp.concatenate(scaled, axis=1)
    scale = lax.rsqrt(jnp.sum(total, axis=1, keepdims=True) / (blocks * lanes) + eps)
    gate = jnp.dot(scaled, gate_ref[0], preferred_element_type=jnp.float32) * scale
    upper = jnp.dot(scaled, up_ref[0], preferred_element_type=jnp.float32) * scale
    gate = jnp.minimum(gate, limit)
    upper = jnp.clip(upper, -limit, limit)
    active = ((upper + 1.0) * gate * jax.nn.sigmoid(alpha * gate)).astype(jnp.bfloat16)
    result = jnp.dot(active, down_ref[0], preferred_element_type=jnp.float32).astype(jnp.bfloat16)
    for t in range(blocks):
        out_ref[t] = result[:, t * lanes : (t + 1) * lanes]


def vmem():
    return pl.BlockSpec(memory_space=pltpu.VMEM)


def local(kernel, name, out_shape, *args, scalars=0, flops=0):
    single = not isinstance(out_shape, list)
    specs = [pl.BlockSpec(memory_space=pltpu.SMEM)] * scalars + [vmem()] * (len(args) - scalars)
    return pl.pallas_call(
        kernel,
        in_specs=specs,
        out_specs=vmem() if single else [vmem()] * len(out_shape),
        out_shape=out_shape,
        compiler_params=pltpu.CompilerParams(vmem_limit_bytes=LIMIT),
        cost_estimate=pl.CostEstimate(flops=flops, bytes_accessed=0, transcendentals=0),
        name=name,
    )(*args)


def exchange(x, axis):
    return lax.all_to_all(x, axis, 0, 0, tiled=True)


def body(
    resid,
    attn_gain,
    w_query,
    w_key,
    w_value,
    key_cache,
    value_cache,
    key_bias,
    lengths,
    mix_gain,
    w_out,
    ffn_gain,
    route_experts,
    route_weights,
    w_gate,
    w_up,
    w_down,
):
    blocks = lax.axis_size(TP)
    groups = lax.axis_size("ep")
    rows, lanes = resid.shape
    heads = mix_gain.shape[0]
    items = groups * CAP
    bf16 = jnp.bfloat16
    shape = jax.ShapeDtypeStruct
    new = shape((rows, heads), bf16)
    experts = route_experts.T
    copies = local(copies_kernel, "copies", shape((blocks, rows, lanes), bf16), resid, flops=LONG)
    parts = exchange(copies, TP)
    new_keys, new_values, partial_branch = local(
        attend_kernel,
        "attend",
        [new, new, shape((blocks, 2 * rows, lanes), bf16)],
        lengths,
        parts,
        attn_gain.reshape(blocks, lanes),
        w_query.T,
        w_key.T,
        w_value.T,
        key_cache,
        value_cache,
        key_bias,
        mix_gain.reshape(1, heads),
        w_out,
        scalars=1,
    )
    middle, outgoing = local(
        middle_kernel,
        "middle",
        [shape((rows, lanes), jnp.float32), shape((groups, SLOTS, lanes), bf16)],
        exchange(partial_branch, TP),
        resid,
        experts,
        flops=SHORT,
    )
    held = local(
        spread_kernel,
        "spread",
        shape((blocks, items, lanes), bf16),
        exchange(outgoing, "ep"),
        flops=SHORT,
    )
    partial_out = local(
        expert_kernel,
        "expert",
        shape((blocks, items, lanes), bf16),
        exchange(held, TP),
        ffn_gain.reshape(blocks, lanes),
        w_gate,
        w_up,
        w_down,
    )
    result = local(
        total_kernel,
        "total",
        shape((groups, SLOTS, lanes), bf16),
        exchange(partial_out, TP),
        flops=SHORT,
    )
    mixed = local(
        mixture_kernel,
        "mixture",
        shape((rows, lanes), bf16),
        exchange(result, "ep"),
        middle,
        experts,
        route_weights.T,
    )
    return (mixed, new_keys, new_values)


def solution(mesh):
    torus = Mesh(mesh.devices.reshape(mesh.shape["ep"], 4, 4), ("ep", "tp_0", "tp_1"))
    in_specs = (
        P("ep", TP),
        P(),
        P(None, TP),
        P(None, TP),
        P(None, TP),
        P("ep", TP, None, None),
        P("ep", TP, None, None),
        P("ep", TP, None),
        P("ep"),
        P(TP),
        P(TP, None),
        P(),
        P("ep", None),
        P("ep", None),
        P("ep", None, TP),
        P("ep", None, TP),
        P("ep", TP, None),
    )
    out_specs = (P("ep", TP), P("ep", TP), P("ep", TP))
    return jax.shard_map(body, mesh=torus, in_specs=in_specs, out_specs=out_specs, check_vma=False)
```

```python
import jax
import jax.numpy as jnp
from jax import lax
from jax.experimental import pallas as pl
from jax.experimental.pallas import tpu as pltpu
from jax.sharding import Mesh
from jax.sharding import PartitionSpec as P

TP = ("tp_0", "tp_1")
EP = ("ep_1", "ep_0")
CORES = 2

eps = 1e-06
limit = 7.0
alpha = 1.702
LANES = 128
SLOTS = 4
CAP = 3
LIMIT = 16 * 1024 * 1024
LONG = 4 * 10**10
SHORT = 10**9


def project(rows, weight_ref):
    return lax.dot_general(
        rows, weight_ref[...], (((1,), (1,)), ((), ())), preferred_element_type=jnp.float32
    ).astype(jnp.bfloat16)


def chosen_slots(experts_ref, slots):
    top, rows = experts_ref.shape
    slot = lax.broadcasted_iota(jnp.int32, (slots, rows), 0)
    block = slot // SLOTS
    chips = slots // SLOTS // CORES
    expert = block % chips * CORES + block // chips
    hits = [experts_ref[k : k + 1, :] == expert for k in range(top)]
    named = hits[0]
    for hit in hits[1:]:
        named = named | hit
    first = lax.broadcasted_iota(jnp.int32, (rows, rows), 0)
    second = lax.broadcasted_iota(jnp.int32, (rows, rows), 1)
    earlier = (first < second).astype(jnp.bfloat16)
    rank = jnp.dot(
        named.astype(jnp.bfloat16), earlier, preferred_element_type=jnp.float32
    ).astype(jnp.int32)
    return hits, named & (rank == slot % SLOTS)


def attend_kernel(parts_ref, lengths_ref, gain_ref, mix_ref, experts_ref, share_ref, wq_ref,
                  wk_ref, wv_ref, key_ref, value_ref, bias_ref, wout_ref, new_key_ref,
                  new_value_ref, out_ref, placed_ref, high_ref, low_ref, fresh_ref, sems):
    blocks, rows, lanes = parts_ref.shape
    heads = key_ref.shape[2]
    cache = key_ref.shape[3]
    xs = [parts_ref[t].astype(jnp.float32) for t in range(blocks)]
    total = xs[0] * xs[0]
    for x in xs[1:]:
        total = total + x * x
    width = blocks * lanes
    scale = lax.rsqrt(jnp.sum(total, axis=1, keepdims=True) / width + eps)
    normed = jnp.concatenate(
        [(xs[t] * scale * gain_ref[t : t + 1, :]).astype(jnp.bfloat16) for t in range(blocks)],
        axis=1,
    )
    query = project(normed, wq_ref).astype(jnp.float32)
    fresh_ref[0] = project(normed, wk_ref)
    fresh_ref[1] = project(normed, wv_ref)
    stores = [
        pltpu.make_async_copy(fresh_ref.at[i], new_ref, sems.at[i])
        for i, new_ref in enumerate((new_key_ref, new_value_ref))
    ]
    for store in stores:
        store.start()
    spread = jnp.concatenate([query] * rows, axis=1)
    row = lax.broadcasted_iota(jnp.int32, spread.shape, 0)
    own = lax.broadcasted_iota(jnp.int32, spread.shape, 1) // heads == row
    spread = jnp.where(own, spread, 0.0).astype(jnp.bfloat16)
    keys = key_ref[:, 0].reshape(rows * heads, cache)
    scores = jnp.dot(spread, keys, preferred_element_type=jnp.float32) * heads ** (-0.5)
    scores = scores + bias_ref[:, 0, :]
    diagonal = lax.broadcasted_iota(jnp.int32, (rows, rows), 0) == lax.broadcasted_iota(
        jnp.int32, (rows, rows), 1
    )
    counts = lengths_ref[...].astype(jnp.float32)
    length = jnp.sum(jnp.where(diagonal, counts, 0.0), axis=1, keepdims=True).astype(jnp.int32)
    live = lax.broadcasted_iota(jnp.int32, (rows, cache), 1) < length
    soft = jnp.maximum(scores, 0.0) + jnp.log1p(jnp.exp(-jnp.abs(scores)))
    drop = jnp.where(live, soft, 0.0)
    chunks = cache // lanes
    stacked = jnp.concatenate([drop[:, c * lanes : (c + 1) * lanes] for c in range(chunks)], axis=0)
    below = lax.broadcasted_iota(jnp.int32, (lanes, lanes), 0)
    across = lax.broadcasted_iota(jnp.int32, (lanes, lanes), 1)
    later = (below > across).astype(jnp.bfloat16)
    high = stacked.astype(jnp.bfloat16)
    rest = stacked - high.astype(jnp.float32)
    middle = rest.astype(jnp.bfloat16)
    low = (rest - middle.astype(jnp.float32)).astype(jnp.bfloat16)
    after = (
        jnp.dot(high, later, preferred_element_type=jnp.float32)
        + jnp.dot(middle, later, preferred_element_type=jnp.float32)
        + jnp.dot(low, later, preferred_element_type=jnp.float32)
    )
    sums = jnp.sum(stacked, axis=1, keepdims=True)
    running = jnp.zeros((rows, 1), jnp.float32)
    pieces = [None] * chunks
    for c in reversed(range(chunks)):
        pieces[c] = after[c * rows : (c + 1) * rows] + running
        running = running + sums[c * rows : (c + 1) * rows]
    after = jnp.concatenate(pieces, axis=1)
    weights = jnp.where(live, jnp.exp(scores - soft - after), 0.0).astype(jnp.bfloat16)
    values = value_ref[:, 0].reshape(rows * heads, cache)
    crossed = lax.dot_general(
        weights, values, (((1,), (1,)), ((), ())), preferred_element_type=jnp.float32
    )
    crossed = jnp.where(own, crossed, 0.0)
    folded = crossed[:, :lanes]
    for c in range(1, crossed.shape[1] // lanes):
        folded = folded + crossed[:, c * lanes : (c + 1) * lanes]
    square = jnp.sum(folded * folded, axis=1, keepdims=True)
    attended = folded[:, :heads] + folded[:, heads : 2 * heads]
    ready = (attended * mix_ref[...]).astype(jnp.bfloat16)
    branch = jnp.dot(ready, wout_ref[...], preferred_element_type=jnp.float32)
    top = square.astype(jnp.bfloat16).astype(jnp.float32)
    half = lax.broadcasted_iota(jnp.int32, (rows, lanes), 1) < lanes // 2
    tail = jnp.where(half, top, square - top)
    for t in range(blocks):
        both = jnp.concatenate([branch[:, t * lanes : (t + 1) * lanes], tail], axis=0)
        out_ref[t] = both.astype(jnp.bfloat16)
    hits, placed = chosen_slots(experts_ref, placed_ref.shape[0])
    share = share_ref[...]
    share = share / jnp.sum(share, axis=0, keepdims=True)
    weight = jnp.where(hits[0], share[:1, :], 0.0)
    for k in range(1, len(hits)):
        weight = weight + jnp.where(hits[k], share[k : k + 1, :], 0.0)
    weight = jnp.where(placed, weight, 0.0)
    high = weight.astype(jnp.bfloat16)
    placed_ref[...] = placed.astype(jnp.bfloat16)
    high_ref[...] = high
    low_ref[...] = (weight - high.astype(jnp.float32)).astype(jnp.bfloat16)
    for store in stores:
        store.wait()


def copies_kernel(*refs):
    count = (len(refs) - 1) // 2
    sources, targets, sems = refs[:count], refs[count : 2 * count], refs[2 * count]
    out_ref = targets[0]
    loads = [
        pltpu.make_async_copy(source, target, sems.at[i])
        for i, (source, target) in enumerate(zip(sources, (out_ref.at[0], *targets[1:])))
    ]
    for load in loads:
        load.start()
    loads[0].wait()
    row = out_ref[0]
    for t in range(1, out_ref.shape[0]):
        out_ref[t] = row
    for load in loads[1:]:
        load.wait()


def middle_kernel(parts_ref, resid_ref, placed_ref, middle_ref, out_ref):
    blocks, both, lanes = parts_ref.shape
    rows = both // 2
    total = parts_ref[0].astype(jnp.float32)
    for t in range(1, blocks):
        total = total + parts_ref[t].astype(jnp.float32)
    square = total[rows:, :1] + total[rows:, lanes - 1 :]
    channels = blocks * (lanes // 2)
    scale = lax.rsqrt(square / channels + eps)
    middle = resid_ref[...].astype(jnp.float32) + total[:rows] * scale
    middle_ref[...] = middle
    out = jnp.dot(
        placed_ref[...], middle.astype(jnp.bfloat16), preferred_element_type=jnp.float32
    )
    out_ref[...] = out.reshape(out_ref.shape).astype(jnp.bfloat16)


def packing(items, slots):
    item = lax.broadcasted_iota(jnp.int32, (items, slots), 0)
    slot = lax.broadcasted_iota(jnp.int32, (items, slots), 1)
    return (item // CAP * SLOTS + item % CAP == slot).astype(jnp.bfloat16)


def spread_kernel(arrived_ref, out_ref):
    blocks, items, lanes = out_ref.shape
    groups, slots, _ = arrived_ref.shape
    arrived = arrived_ref[...].astype(jnp.float32).reshape(groups * slots, lanes)
    held = jnp.dot(
        packing(items, groups * slots),
        arrived.astype(jnp.bfloat16),
        preferred_element_type=jnp.float32,
    ).astype(jnp.bfloat16)
    for t in range(blocks):
        out_ref[t] = held


def total_kernel(parts_ref, out_ref):
    blocks, items, lanes = parts_ref.shape
    groups, slots, _ = out_ref.shape
    total = parts_ref[0].astype(jnp.float32)
    for t in range(1, blocks):
        total = total + parts_ref[t].astype(jnp.float32)
    spaced = lax.dot_general(
        packing(items, groups * slots),
        total.astype(jnp.bfloat16),
        (((0,), (0,)), ((), ())),
        preferred_element_type=jnp.float32,
    )
    out_ref[...] = spaced.reshape(groups, slots, lanes).astype(jnp.bfloat16)


def mixture_kernel(returned_ref, middle_ref, high_ref, low_ref, out_ref):
    groups, slots, lanes = returned_ref.shape
    returned = returned_ref[...].astype(jnp.float32).reshape(groups * slots, lanes)
    returned = returned.astype(jnp.bfloat16)
    mixture = sum(
        lax.dot_general(
            part[...], returned, (((0,), (0,)), ((), ())), preferred_element_type=jnp.float32
        )
        for part in (high_ref, low_ref)
    )
    out_ref[...] = (middle_ref[...] + mixture).astype(jnp.bfloat16)


def expert_kernel(rows_ref, gain_ref, gate_ref, up_ref, down_ref, out_ref):
    blocks, rows, lanes = rows_ref.shape
    total = jnp.zeros((rows, lanes), jnp.float32)
    scaled = []
    for t in range(blocks):
        x = rows_ref[t].astype(jnp.float32)
        total = total + x * x
        scaled.append((x * gain_ref[t : t + 1, :]).astype(jnp.bfloat16))
    scaled = jnp.concatenate(scaled, axis=1)
    scale = lax.rsqrt(jnp.sum(total, axis=1, keepdims=True) / (blocks * lanes) + eps)
    gate = jnp.dot(scaled, gate_ref[0], preferred_element_type=jnp.float32) * scale
    upper = jnp.dot(scaled, up_ref[0], preferred_element_type=jnp.float32) * scale
    gate = jnp.minimum(gate, limit)
    upper = jnp.clip(upper, -limit, limit)
    active = ((upper + 1.0) * gate * jax.nn.sigmoid(alpha * gate)).astype(jnp.bfloat16)
    result = jnp.dot(active, down_ref[0], preferred_element_type=jnp.float32).astype(jnp.bfloat16)
    for t in range(blocks):
        out_ref[t] = result[:, t * lanes : (t + 1) * lanes]


def local(kernel, name, out_shape, *args, flops=0, far_in=0, far_out=0, scratch=()):
    def places(count, far):
        return [pl.BlockSpec(memory_space=pltpu.HBM)] * far + [
            pl.BlockSpec(memory_space=pltpu.VMEM)
        ] * (count - far)

    single = not isinstance(out_shape, list)
    outs = places(1 if single else len(out_shape), far_out)
    return pl.pallas_call(
        kernel,
        in_specs=places(len(args), far_in),
        out_specs=outs[0] if single else outs,
        out_shape=out_shape,
        scratch_shapes=scratch,
        compiler_params=pltpu.CompilerParams(vmem_limit_bytes=LIMIT),
        cost_estimate=pl.CostEstimate(flops=flops, bytes_accessed=0, transcendentals=0),
        name=name,
    )(*[pltpu.with_memory_space_constraint(x, pltpu.HBM) for x in args[:far_in]], *args[far_in:])


def exchange(x, axis):
    return lax.all_to_all(x, axis, 0, 0, tiled=True)


def body(
    resid,
    attn_gain,
    w_query,
    w_key,
    w_value,
    key_cache,
    value_cache,
    key_bias,
    lengths,
    mix_gain,
    w_out,
    ffn_gain,
    route_experts,
    route_weights,
    w_gate,
    w_up,
    w_down,
):
    blocks = lax.axis_size(TP)
    groups = lax.axis_size(EP)
    rows, lanes = resid.shape
    heads = mix_gain.shape[0]
    items = groups * CAP
    bf16 = jnp.bfloat16
    shape = jax.ShapeDtypeStruct
    slots = groups * SLOTS
    new = shape((rows, heads), bf16)
    small = (
        lengths.reshape(1, rows),
        attn_gain.reshape(blocks, lanes),
        mix_gain.reshape(1, heads),
        route_experts.T,
        route_weights.T,
    )
    copies, *small = local(
        copies_kernel,
        "copies",
        [shape((blocks, rows, lanes), bf16)] + [shape(x.shape, x.dtype) for x in small],
        resid,
        *small,
        flops=LONG,
        far_in=1 + len(small),
        scratch=[pltpu.SemaphoreType.DMA((1 + len(small),))],
    )
    new_keys, new_values, partial_branch, placed, high, low = local(
        attend_kernel,
        "attend",
        [new, new, shape((blocks, 2 * rows, lanes), bf16)] + [shape((slots, rows), bf16)] * 3,
        exchange(copies, TP),
        *small,
        w_query.T,
        w_key.T,
        w_value.T,
        key_cache,
        value_cache,
        key_bias,
        w_out,
        far_out=2,
        scratch=[pltpu.VMEM((2, rows, heads), bf16), pltpu.SemaphoreType.DMA((2,))],
    )
    middle, outgoing = local(
        middle_kernel,
        "middle",
        [shape((rows, lanes), jnp.float32), shape((groups, SLOTS, lanes), bf16)],
        exchange(partial_branch, TP),
        resid,
        placed,
        flops=SHORT,
    )
    held = local(
        spread_kernel,
        "spread",
        shape((blocks, items, lanes), bf16),
        exchange(outgoing, EP),
        flops=SHORT,
    )
    partial_out = local(
        expert_kernel,
        "expert",
        shape((blocks, items, lanes), bf16),
        exchange(held, TP),
        ffn_gain.reshape(blocks, lanes),
        w_gate,
        w_up,
        w_down,
    )
    result = local(
        total_kernel,
        "total",
        shape((groups, SLOTS, lanes), bf16),
        exchange(partial_out, TP),
        flops=SHORT,
    )
    mixed = local(
        mixture_kernel,
        "mixture",
        shape((rows, lanes), bf16),
        exchange(result, EP),
        middle,
        high,
        low,
    )
    return (mixed, new_keys, new_values)


def solution(mesh):
    torus = Mesh(
        mesh.devices.reshape(mesh.shape["ep"] // CORES, CORES, 4, 4),
        ("ep_0", "ep_1", "tp_0", "tp_1"),
    )
    rows = ("ep_0", "ep_1")
    in_specs = (
        P(rows, TP),
        P(),
        P(None, TP),
        P(None, TP),
        P(None, TP),
        P(rows, TP, None, None),
        P(rows, TP, None, None),
        P(rows, TP, None),
        P(rows),
        P(TP),
        P(TP, None),
        P(),
        P(rows, None),
        P(rows, None),
        P(rows, None, TP),
        P(rows, None, TP),
        P(rows, TP, None),
    )
    out_specs = (P(rows, TP), P(rows, TP), P(rows, TP))
    return jax.shard_map(body, mesh=torus, in_specs=in_specs, out_specs=out_specs, check_vma=False)
```

```python
import jax
import jax.numpy as jnp
from jax import lax
from jax.experimental import pallas as pl
from jax.experimental.pallas import tpu as pltpu
from jax.sharding import Mesh
from jax.sharding import PartitionSpec as P

TP = ("tp_0", "tp_1")
EP = ("ep_1", "ep_0")
CORES = 2

eps = 1e-06
limit = 7.0
alpha = 1.702
LANES = 128
SLOTS = 4
CAP = 3
LIMIT = 16 * 1024 * 1024
LONG = 4 * 10**10
SHORT = 10**9


def project(rows, weight_ref):
    return lax.dot_general(
        rows, weight_ref[...], (((1,), (1,)), ((), ())), preferred_element_type=jnp.float32
    ).astype(jnp.bfloat16)


def chosen_slots(experts_ref, slots):
    top, rows = experts_ref.shape
    slot = lax.broadcasted_iota(jnp.int32, (slots, rows), 0)
    block = slot // SLOTS
    chips = slots // SLOTS // CORES
    expert = block % chips * CORES + block // chips
    hits = [experts_ref[k : k + 1, :] == expert for k in range(top)]
    named = hits[0]
    for hit in hits[1:]:
        named = named | hit
    first = lax.broadcasted_iota(jnp.int32, (rows, rows), 0)
    second = lax.broadcasted_iota(jnp.int32, (rows, rows), 1)
    earlier = (first < second).astype(jnp.bfloat16)
    rank = jnp.dot(
        named.astype(jnp.bfloat16), earlier, preferred_element_type=jnp.float32
    ).astype(jnp.int32)
    return hits, named & (rank == slot % SLOTS)


def attend_kernel(parts_ref, lengths_ref, gain_ref, mix_ref, experts_ref, share_ref, wq_ref,
                  wk_ref, wv_ref, key_ref, value_ref, bias_ref, wout_ref, new_key_ref,
                  new_value_ref, out_ref, placed_ref, high_ref, low_ref, fresh_ref, sems):
    blocks, rows, lanes = parts_ref.shape
    heads = key_ref.shape[2]
    cache = key_ref.shape[3]
    xs = [parts_ref[t].astype(jnp.float32) for t in range(blocks)]
    total = xs[0] * xs[0]
    for x in xs[1:]:
        total = total + x * x
    width = blocks * lanes
    scale = lax.rsqrt(jnp.sum(total, axis=1, keepdims=True) / width + eps)
    normed = jnp.concatenate(
        [(xs[t] * scale * gain_ref[t : t + 1, :]).astype(jnp.bfloat16) for t in range(blocks)],
        axis=1,
    )
    query = project(normed, wq_ref).astype(jnp.float32)
    fresh_ref[0] = project(normed, wk_ref)
    fresh_ref[1] = project(normed, wv_ref)
    stores = [
        pltpu.make_async_copy(fresh_ref.at[i], new_ref, sems.at[i])
        for i, new_ref in enumerate((new_key_ref, new_value_ref))
    ]
    for store in stores:
        store.start()
    spread = jnp.concatenate([query] * rows, axis=1)
    row = lax.broadcasted_iota(jnp.int32, spread.shape, 0)
    own = lax.broadcasted_iota(jnp.int32, spread.shape, 1) // heads == row
    spread = jnp.where(own, spread, 0.0).astype(jnp.bfloat16)
    keys = key_ref[:, 0].reshape(rows * heads, cache)
    scores = jnp.dot(spread, keys, preferred_element_type=jnp.float32) * heads ** (-0.5)
    scores = scores + bias_ref[:, 0, :]
    diagonal = lax.broadcasted_iota(jnp.int32, (rows, rows), 0) == lax.broadcasted_iota(
        jnp.int32, (rows, rows), 1
    )
    counts = lengths_ref[...].astype(jnp.float32)
    length = jnp.sum(jnp.where(diagonal, counts, 0.0), axis=1, keepdims=True).astype(jnp.int32)
    live = lax.broadcasted_iota(jnp.int32, (rows, cache), 1) < length
    soft = jnp.maximum(scores, 0.0) + jnp.log1p(jnp.exp(-jnp.abs(scores)))
    drop = jnp.where(live, soft, 0.0)
    chunks = cache // lanes
    stacked = jnp.concatenate([drop[:, c * lanes : (c + 1) * lanes] for c in range(chunks)], axis=0)
    below = lax.broadcasted_iota(jnp.int32, (lanes, lanes), 0)
    across = lax.broadcasted_iota(jnp.int32, (lanes, lanes), 1)
    later = (below > across).astype(jnp.bfloat16)
    high = stacked.astype(jnp.bfloat16)
    rest = stacked - high.astype(jnp.float32)
    middle = rest.astype(jnp.bfloat16)
    low = (rest - middle.astype(jnp.float32)).astype(jnp.bfloat16)
    after = (
        jnp.dot(high, later, preferred_element_type=jnp.float32)
        + jnp.dot(middle, later, preferred_element_type=jnp.float32)
        + jnp.dot(low, later, preferred_element_type=jnp.float32)
    )
    sums = jnp.sum(stacked, axis=1, keepdims=True)
    running = jnp.zeros((rows, 1), jnp.float32)
    pieces = [None] * chunks
    for c in reversed(range(chunks)):
        pieces[c] = after[c * rows : (c + 1) * rows] + running
        running = running + sums[c * rows : (c + 1) * rows]
    after = jnp.concatenate(pieces, axis=1)
    weights = jnp.where(live, jnp.exp(scores - soft - after), 0.0).astype(jnp.bfloat16)
    values = value_ref[:, 0].reshape(rows * heads, cache)
    crossed = lax.dot_general(
        weights, values, (((1,), (1,)), ((), ())), preferred_element_type=jnp.float32
    )
    crossed = jnp.where(own, crossed, 0.0)
    folded = crossed[:, :lanes]
    for c in range(1, crossed.shape[1] // lanes):
        folded = folded + crossed[:, c * lanes : (c + 1) * lanes]
    square = jnp.sum(folded * folded, axis=1, keepdims=True)
    attended = folded[:, :heads] + folded[:, heads : 2 * heads]
    ready = (attended * mix_ref[...]).astype(jnp.bfloat16)
    branch = jnp.dot(ready, wout_ref[...], preferred_element_type=jnp.float32)
    top = square.astype(jnp.bfloat16).astype(jnp.float32)
    half = lax.broadcasted_iota(jnp.int32, (rows, lanes), 1) < lanes // 2
    tail = jnp.where(half, top, square - top)
    for t in range(blocks):
        both = jnp.concatenate([branch[:, t * lanes : (t + 1) * lanes], tail], axis=0)
        out_ref[t] = both.astype(jnp.bfloat16)
    hits, placed = chosen_slots(experts_ref, placed_ref.shape[0])
    share = share_ref[...]
    share = share / jnp.sum(share, axis=0, keepdims=True)
    weight = jnp.where(hits[0], share[:1, :], 0.0)
    for k in range(1, len(hits)):
        weight = weight + jnp.where(hits[k], share[k : k + 1, :], 0.0)
    weight = jnp.where(placed, weight, 0.0)
    high = weight.astype(jnp.bfloat16)
    placed_ref[...] = placed.astype(jnp.bfloat16)
    high_ref[...] = high
    low_ref[...] = (weight - high.astype(jnp.float32)).astype(jnp.bfloat16)
    for store in stores:
        store.wait()


def load_kernel(*refs):
    count = len(refs) // 2
    sources, targets, sems = refs[:count], refs[count : 2 * count], refs[2 * count]
    loads = [
        pltpu.make_async_copy(source, target, sems.at[i])
        for i, (source, target) in enumerate(zip(sources, targets))
    ]
    for load in loads:
        load.start()
    for load in loads:
        load.wait()


def copies_kernel(row_ref, out_ref):
    row = row_ref[...]
    for t in range(out_ref.shape[0]):
        out_ref[t] = row


def middle_kernel(parts_ref, resid_ref, placed_ref, middle_ref, out_ref):
    blocks, both, lanes = parts_ref.shape
    rows = both // 2
    total = parts_ref[0].astype(jnp.float32)
    for t in range(1, blocks):
        total = total + parts_ref[t].astype(jnp.float32)
    square = total[rows:, :1] + total[rows:, lanes - 1 :]
    channels = blocks * (lanes // 2)
    scale = lax.rsqrt(square / channels + eps)
    middle = resid_ref[...].astype(jnp.float32) + total[:rows] * scale
    middle_ref[...] = middle
    out = jnp.dot(
        placed_ref[...], middle.astype(jnp.bfloat16), preferred_element_type=jnp.float32
    )
    out_ref[...] = out.reshape(out_ref.shape).astype(jnp.bfloat16)


def packing(items, slots):
    item = lax.broadcasted_iota(jnp.int32, (items, slots), 0)
    slot = lax.broadcasted_iota(jnp.int32, (items, slots), 1)
    return (item // CAP * SLOTS + item % CAP == slot).astype(jnp.bfloat16)


def spread_kernel(arrived_ref, out_ref):
    blocks, items, lanes = out_ref.shape
    groups, slots, _ = arrived_ref.shape
    arrived = arrived_ref[...].astype(jnp.float32).reshape(groups * slots, lanes)
    held = jnp.dot(
        packing(items, groups * slots),
        arrived.astype(jnp.bfloat16),
        preferred_element_type=jnp.float32,
    ).astype(jnp.bfloat16)
    for t in range(blocks):
        out_ref[t] = held


def total_kernel(parts_ref, out_ref):
    blocks, items, lanes = parts_ref.shape
    groups, slots, _ = out_ref.shape
    total = parts_ref[0].astype(jnp.float32)
    for t in range(1, blocks):
        total = total + parts_ref[t].astype(jnp.float32)
    spaced = lax.dot_general(
        packing(items, groups * slots),
        total.astype(jnp.bfloat16),
        (((0,), (0,)), ((), ())),
        preferred_element_type=jnp.float32,
    )
    out_ref[...] = spaced.reshape(groups, slots, lanes).astype(jnp.bfloat16)


def mixture_kernel(returned_ref, middle_ref, high_ref, low_ref, out_ref):
    groups, slots, lanes = returned_ref.shape
    returned = returned_ref[...].astype(jnp.float32).reshape(groups * slots, lanes)
    returned = returned.astype(jnp.bfloat16)
    mixture = sum(
        lax.dot_general(
            part[...], returned, (((0,), (0,)), ((), ())), preferred_element_type=jnp.float32
        )
        for part in (high_ref, low_ref)
    )
    out_ref[...] = (middle_ref[...] + mixture).astype(jnp.bfloat16)


def expert_kernel(rows_ref, gain_ref, gate_ref, up_ref, down_ref, out_ref):
    blocks, rows, lanes = rows_ref.shape
    total = jnp.zeros((rows, lanes), jnp.float32)
    scaled = []
    for t in range(blocks):
        x = rows_ref[t].astype(jnp.float32)
        total = total + x * x
        scaled.append((x * gain_ref[t : t + 1, :]).astype(jnp.bfloat16))
    scaled = jnp.concatenate(scaled, axis=1)
    scale = lax.rsqrt(jnp.sum(total, axis=1, keepdims=True) / (blocks * lanes) + eps)
    gate = jnp.dot(scaled, gate_ref[0], preferred_element_type=jnp.float32) * scale
    upper = jnp.dot(scaled, up_ref[0], preferred_element_type=jnp.float32) * scale
    gate = jnp.minimum(gate, limit)
    upper = jnp.clip(upper, -limit, limit)
    active = ((upper + 1.0) * gate * jax.nn.sigmoid(alpha * gate)).astype(jnp.bfloat16)
    result = jnp.dot(active, down_ref[0], preferred_element_type=jnp.float32).astype(jnp.bfloat16)
    for t in range(blocks):
        out_ref[t] = result[:, t * lanes : (t + 1) * lanes]


def local(kernel, name, out_shape, *args, flops=0, far_in=0, far_out=0, scratch=()):
    def places(count, far):
        return [pl.BlockSpec(memory_space=pltpu.HBM)] * far + [
            pl.BlockSpec(memory_space=pltpu.VMEM)
        ] * (count - far)

    single = not isinstance(out_shape, list)
    outs = places(1 if single else len(out_shape), far_out)
    return pl.pallas_call(
        kernel,
        in_specs=places(len(args), far_in),
        out_specs=outs[0] if single else outs,
        out_shape=out_shape,
        scratch_shapes=scratch,
        compiler_params=pltpu.CompilerParams(vmem_limit_bytes=LIMIT),
        cost_estimate=pl.CostEstimate(flops=flops, bytes_accessed=0, transcendentals=0),
        name=name,
    )(*[pltpu.with_memory_space_constraint(x, pltpu.HBM) for x in args[:far_in]], *args[far_in:])


def exchange(x, axis):
    return lax.all_to_all(x, axis, 0, 0, tiled=True)


def body(
    resid,
    attn_gain,
    w_query,
    w_key,
    w_value,
    key_cache,
    value_cache,
    key_bias,
    lengths,
    mix_gain,
    w_out,
    ffn_gain,
    route_experts,
    route_weights,
    w_gate,
    w_up,
    w_down,
):
    blocks = lax.axis_size(TP)
    groups = lax.axis_size(EP)
    rows, lanes = resid.shape
    heads = mix_gain.shape[0]
    items = groups * CAP
    bf16 = jnp.bfloat16
    shape = jax.ShapeDtypeStruct
    slots = groups * SLOTS
    new = shape((rows, heads), bf16)
    small = (
        resid,
        lengths.reshape(1, rows),
        attn_gain.reshape(blocks, lanes),
        mix_gain.reshape(1, heads),
        route_experts.T,
        route_weights.T,
    )
    near, *small = local(
        load_kernel,
        "load",
        [shape(x.shape, x.dtype) for x in small],
        *small,
        far_in=len(small),
        scratch=[pltpu.SemaphoreType.DMA((len(small),))],
    )
    copies = local(
        copies_kernel, "copies", shape((blocks, rows, lanes), bf16), near, flops=LONG
    )
    new_keys, new_values, partial_branch, placed, high, low = local(
        attend_kernel,
        "attend",
        [new, new, shape((blocks, 2 * rows, lanes), bf16)] + [shape((slots, rows), bf16)] * 3,
        exchange(copies, TP),
        *small,
        w_query.T,
        w_key.T,
        w_value.T,
        key_cache,
        value_cache,
        key_bias,
        w_out,
        far_out=2,
        scratch=[pltpu.VMEM((2, rows, heads), bf16), pltpu.SemaphoreType.DMA((2,))],
    )
    middle, outgoing = local(
        middle_kernel,
        "middle",
        [shape((rows, lanes), jnp.float32), shape((groups, SLOTS, lanes), bf16)],
        exchange(partial_branch, TP),
        near,
        placed,
        flops=SHORT,
    )
    held = local(
        spread_kernel,
        "spread",
        shape((blocks, items, lanes), bf16),
        exchange(outgoing, EP),
        flops=SHORT,
    )
    partial_out = local(
        expert_kernel,
        "expert",
        shape((blocks, items, lanes), bf16),
        exchange(held, TP),
        ffn_gain.reshape(blocks, lanes),
        w_gate,
        w_up,
        w_down,
    )
    result = local(
        total_kernel,
        "total",
        shape((groups, SLOTS, lanes), bf16),
        exchange(partial_out, TP),
        flops=SHORT,
    )
    mixed = local(
        mixture_kernel,
        "mixture",
        shape((rows, lanes), bf16),
        exchange(result, EP),
        middle,
        high,
        low,
    )
    return (mixed, new_keys, new_values)


def solution(mesh):
    torus = Mesh(
        mesh.devices.reshape(mesh.shape["ep"] // CORES, CORES, 4, 4),
        ("ep_0", "ep_1", "tp_0", "tp_1"),
    )
    rows = ("ep_0", "ep_1")
    in_specs = (
        P(rows, TP),
        P(),
        P(None, TP),
        P(None, TP),
        P(None, TP),
        P(rows, TP, None, None),
        P(rows, TP, None, None),
        P(rows, TP, None),
        P(rows),
        P(TP),
        P(TP, None),
        P(),
        P(rows, None),
        P(rows, None),
        P(rows, None, TP),
        P(rows, None, TP),
        P(rows, TP, None),
    )
    out_specs = (P(rows, TP), P(rows, TP), P(rows, TP))
    return jax.shard_map(body, mesh=torus, in_specs=in_specs, out_specs=out_specs, check_vma=False)
```

```python
import jax
import jax.numpy as jnp
from jax import lax
from jax.experimental import pallas as pl
from jax.experimental.pallas import tpu as pltpu
from jax.sharding import Mesh
from jax.sharding import PartitionSpec as P

TP = ("tp_0", "tp_1", "tp_2")
NEAR = ("tp_0", "tp_2")
EP = ("ep_1", "ep_0")
CORES = 2

eps = 1e-06
limit = 7.0
alpha = 1.702
LANES = 128
SLOTS = 4
CAP = 3
LIMIT = 16 * 1024 * 1024
LONG = 4 * 10**10
SHORT = 10**9


def project(rows, weight_ref):
    return lax.dot_general(
        rows, weight_ref[...], (((1,), (1,)), ((), ())), preferred_element_type=jnp.float32
    ).astype(jnp.bfloat16)


def pair_of(t):
    return t & ~2, t | 2


def chosen_slots(experts_ref, slots):
    top, rows = experts_ref.shape
    slot = lax.broadcasted_iota(jnp.int32, (slots, rows), 0)
    block = slot // SLOTS
    chips = slots // SLOTS // CORES
    expert = block % chips * CORES + block // chips
    hits = [experts_ref[k : k + 1, :] == expert for k in range(top)]
    named = hits[0]
    for hit in hits[1:]:
        named = named | hit
    first = lax.broadcasted_iota(jnp.int32, (rows, rows), 0)
    second = lax.broadcasted_iota(jnp.int32, (rows, rows), 1)
    earlier = (first < second).astype(jnp.bfloat16)
    rank = jnp.dot(
        named.astype(jnp.bfloat16), earlier, preferred_element_type=jnp.float32
    ).astype(jnp.int32)
    return hits, named & (rank == slot % SLOTS)


def attend_kernel(parts_ref, lengths_ref, gain_ref, mix_ref, experts_ref, share_ref, wq_ref,
                  wk_ref, wv_ref, key_ref, value_ref, bias_ref, wout_ref, new_key_ref,
                  new_value_ref, out_ref, placed_ref, high_ref, low_ref, fresh_ref, sems):
    blocks, rows, lanes = parts_ref.shape
    heads = key_ref.shape[2]
    cache = key_ref.shape[3]
    xs = [parts_ref[t].astype(jnp.float32) for t in range(blocks)]
    total = xs[0] * xs[0]
    for x in xs[1:]:
        total = total + x * x
    width = blocks * lanes
    scale = lax.rsqrt(jnp.sum(total, axis=1, keepdims=True) / width + eps)
    normed = jnp.concatenate(
        [(xs[t] * scale * gain_ref[t : t + 1, :]).astype(jnp.bfloat16) for t in range(blocks)],
        axis=1,
    )
    query = project(normed, wq_ref).astype(jnp.float32)
    fresh_ref[0] = project(normed, wk_ref)
    fresh_ref[1] = project(normed, wv_ref)
    stores = [
        pltpu.make_async_copy(fresh_ref.at[i], new_ref, sems.at[i])
        for i, new_ref in enumerate((new_key_ref, new_value_ref))
    ]
    for store in stores:
        store.start()
    spread = jnp.concatenate([query] * rows, axis=1)
    row = lax.broadcasted_iota(jnp.int32, spread.shape, 0)
    own = lax.broadcasted_iota(jnp.int32, spread.shape, 1) // heads == row
    spread = jnp.where(own, spread, 0.0).astype(jnp.bfloat16)
    keys = key_ref[:, 0].reshape(rows * heads, cache)
    scores = jnp.dot(spread, keys, preferred_element_type=jnp.float32) * heads ** (-0.5)
    scores = scores + bias_ref[:, 0, :]
    diagonal = lax.broadcasted_iota(jnp.int32, (rows, rows), 0) == lax.broadcasted_iota(
        jnp.int32, (rows, rows), 1
    )
    counts = lengths_ref[...].astype(jnp.float32)
    length = jnp.sum(jnp.where(diagonal, counts, 0.0), axis=1, keepdims=True).astype(jnp.int32)
    live = lax.broadcasted_iota(jnp.int32, (rows, cache), 1) < length
    soft = jnp.maximum(scores, 0.0) + jnp.log1p(jnp.exp(-jnp.abs(scores)))
    drop = jnp.where(live, soft, 0.0)
    chunks = cache // lanes
    stacked = jnp.concatenate([drop[:, c * lanes : (c + 1) * lanes] for c in range(chunks)], axis=0)
    below = lax.broadcasted_iota(jnp.int32, (lanes, lanes), 0)
    across = lax.broadcasted_iota(jnp.int32, (lanes, lanes), 1)
    later = (below > across).astype(jnp.bfloat16)
    high = stacked.astype(jnp.bfloat16)
    rest = stacked - high.astype(jnp.float32)
    middle = rest.astype(jnp.bfloat16)
    low = (rest - middle.astype(jnp.float32)).astype(jnp.bfloat16)
    after = (
        jnp.dot(high, later, preferred_element_type=jnp.float32)
        + jnp.dot(middle, later, preferred_element_type=jnp.float32)
        + jnp.dot(low, later, preferred_element_type=jnp.float32)
    )
    sums = jnp.sum(stacked, axis=1, keepdims=True)
    running = jnp.zeros((rows, 1), jnp.float32)
    pieces = [None] * chunks
    for c in reversed(range(chunks)):
        pieces[c] = after[c * rows : (c + 1) * rows] + running
        running = running + sums[c * rows : (c + 1) * rows]
    after = jnp.concatenate(pieces, axis=1)
    weights = jnp.where(live, jnp.exp(scores - soft - after), 0.0).astype(jnp.bfloat16)
    values = value_ref[:, 0].reshape(rows * heads, cache)
    crossed = lax.dot_general(
        weights, values, (((1,), (1,)), ((), ())), preferred_element_type=jnp.float32
    )
    crossed = jnp.where(own, crossed, 0.0)
    folded = crossed[:, :lanes]
    for c in range(1, crossed.shape[1] // lanes):
        folded = folded + crossed[:, c * lanes : (c + 1) * lanes]
    square = jnp.sum(folded * folded, axis=1, keepdims=True)
    attended = folded[:, :heads] + folded[:, heads : 2 * heads]
    ready = (attended * mix_ref[...]).astype(jnp.bfloat16)
    branch = jnp.dot(ready, wout_ref[...], preferred_element_type=jnp.float32)
    top = square.astype(jnp.bfloat16).astype(jnp.float32)
    half = lax.broadcasted_iota(jnp.int32, (rows, lanes), 1) < lanes // 2
    tail = jnp.where(half, top, square - top)
    tail = tail.astype(jnp.bfloat16)
    for t in range(blocks):
        low, high = [
            branch[:, i * lanes : (i + 1) * lanes].astype(jnp.bfloat16) for i in pair_of(t)
        ]
        out_ref[t] = jnp.concatenate([low, high, tail], axis=0)
    hits, placed = chosen_slots(experts_ref, placed_ref.shape[0])
    share = share_ref[...]
    share = share / jnp.sum(share, axis=0, keepdims=True)
    weight = jnp.where(hits[0], share[:1, :], 0.0)
    for k in range(1, len(hits)):
        weight = weight + jnp.where(hits[k], share[k : k + 1, :], 0.0)
    weight = jnp.where(placed, weight, 0.0)
    high = weight.astype(jnp.bfloat16)
    placed_ref[...] = placed.astype(jnp.bfloat16)
    high_ref[...] = high
    low_ref[...] = (weight - high.astype(jnp.float32)).astype(jnp.bfloat16)
    for store in stores:
        store.wait()


def load_kernel(*refs):
    count = len(refs) // 2
    sources, targets, sems = refs[:count], refs[count : 2 * count], refs[2 * count]
    loads = [
        pltpu.make_async_copy(source, target, sems.at[i])
        for i, (source, target) in enumerate(zip(sources, targets))
    ]
    for load in loads:
        load.start()
    for load in loads:
        load.wait()


def copies_kernel(row_ref, out_ref):
    row = row_ref[...]
    for t in range(out_ref.shape[0]):
        out_ref[t] = row


def middle_kernel(parts_ref, resid_ref, placed_ref, middle_ref, out_ref):
    blocks, stacked, lanes = parts_ref.shape
    rows = stacked // 3
    total = parts_ref[0].astype(jnp.float32)
    for t in range(1, blocks):
        total = total + parts_ref[t].astype(jnp.float32)
    square = total[2 * rows :, :1] + total[2 * rows :, lanes - 1 :]
    channels = blocks * (lanes // 2)
    scale = lax.rsqrt(square / channels + eps)
    low = lax.axis_index("tp_0") * 4 + lax.axis_index("tp_2")
    pair = [
        resid_ref[low + 2 * i].astype(jnp.float32) + total[i * rows : (i + 1) * rows] * scale
        for i in range(2)
    ]
    middle_ref[...] = jnp.where(lax.axis_index("tp_1") == 0, pair[0], pair[1])
    for i in range(2):
        out = jnp.dot(
            placed_ref[...], pair[i].astype(jnp.bfloat16), preferred_element_type=jnp.float32
        )
        groups = out_ref.shape[0]
        out_ref[:, i * SLOTS : (i + 1) * SLOTS, :] = out.reshape(groups, SLOTS, lanes).astype(
            jnp.bfloat16
        )


def packing(items, slots):
    item = lax.broadcasted_iota(jnp.int32, (items, slots), 0)
    slot = lax.broadcasted_iota(jnp.int32, (items, slots), 1)
    return (item // CAP * SLOTS + item % CAP == slot).astype(jnp.bfloat16)


def spread_kernel(arrived_ref, out_ref):
    blocks, both, lanes = out_ref.shape
    groups = arrived_ref.shape[0]
    pack = packing(both // 2, groups * SLOTS)
    arrived = arrived_ref[...].astype(jnp.float32)
    held = [
        jnp.dot(
            pack,
            arrived[:, i * SLOTS : (i + 1) * SLOTS]
            .reshape(groups * SLOTS, lanes)
            .astype(jnp.bfloat16),
            preferred_element_type=jnp.float32,
        )
        for i in range(2)
    ]
    held = jnp.concatenate(held, axis=0).astype(jnp.bfloat16)
    for t in range(blocks):
        out_ref[t] = held


def total_kernel(parts_ref, out_ref):
    blocks, items, lanes = parts_ref.shape
    groups, slots, _ = out_ref.shape
    total = parts_ref[0].astype(jnp.float32)
    for t in range(1, blocks):
        total = total + parts_ref[t].astype(jnp.float32)
    spaced = lax.dot_general(
        packing(items, groups * slots),
        total.astype(jnp.bfloat16),
        (((0,), (0,)), ((), ())),
        preferred_element_type=jnp.float32,
    )
    out_ref[...] = spaced.reshape(groups, slots, lanes).astype(jnp.bfloat16)


def mixture_kernel(returned_ref, middle_ref, high_ref, low_ref, out_ref):
    groups, slots, lanes = returned_ref.shape
    returned = returned_ref[...].astype(jnp.float32).reshape(groups * slots, lanes)
    returned = returned.astype(jnp.bfloat16)
    mixture = sum(
        lax.dot_general(
            part[...], returned, (((0,), (0,)), ((), ())), preferred_element_type=jnp.float32
        )
        for part in (high_ref, low_ref)
    )
    out_ref[...] = (middle_ref[...] + mixture).astype(jnp.bfloat16)


def expert_kernel(rows_ref, gain_ref, gate_ref, up_ref, down_ref, out_ref):
    blocks, rows, lanes = out_ref.shape
    total = jnp.zeros((rows, lanes), jnp.float32)
    scaled = []
    for t in range(blocks):
        side = t % 4 // 2
        x = rows_ref[t // 4 * 2 + t % 2, side * rows : (side + 1) * rows].astype(jnp.float32)
        total = total + x * x
        scaled.append((x * gain_ref[t : t + 1, :]).astype(jnp.bfloat16))
    scaled = jnp.concatenate(scaled, axis=1)
    scale = lax.rsqrt(jnp.sum(total, axis=1, keepdims=True) / (blocks * lanes) + eps)
    gate = jnp.dot(scaled, gate_ref[0], preferred_element_type=jnp.float32) * scale
    upper = jnp.dot(scaled, up_ref[0], preferred_element_type=jnp.float32) * scale
    gate = jnp.minimum(gate, limit)
    upper = jnp.clip(upper, -limit, limit)
    active = ((upper + 1.0) * gate * jax.nn.sigmoid(alpha * gate)).astype(jnp.bfloat16)
    result = jnp.dot(active, down_ref[0], preferred_element_type=jnp.float32).astype(jnp.bfloat16)
    for t in range(blocks):
        out_ref[t] = result[:, t * lanes : (t + 1) * lanes]


def local(kernel, name, out_shape, *args, flops=0, far_in=0, far_out=0, scratch=()):
    def places(count, far):
        return [pl.BlockSpec(memory_space=pltpu.HBM)] * far + [
            pl.BlockSpec(memory_space=pltpu.VMEM)
        ] * (count - far)

    single = not isinstance(out_shape, list)
    outs = places(1 if single else len(out_shape), far_out)
    return pl.pallas_call(
        kernel,
        in_specs=places(len(args), far_in),
        out_specs=outs[0] if single else outs,
        out_shape=out_shape,
        scratch_shapes=scratch,
        compiler_params=pltpu.CompilerParams(vmem_limit_bytes=LIMIT),
        cost_estimate=pl.CostEstimate(flops=flops, bytes_accessed=0, transcendentals=0),
        name=name,
    )(*[pltpu.with_memory_space_constraint(x, pltpu.HBM) for x in args[:far_in]], *args[far_in:])


def exchange(x, axis):
    return lax.all_to_all(x, axis, 0, 0, tiled=True)


def body(
    resid,
    attn_gain,
    w_query,
    w_key,
    w_value,
    key_cache,
    value_cache,
    key_bias,
    lengths,
    mix_gain,
    w_out,
    ffn_gain,
    route_experts,
    route_weights,
    w_gate,
    w_up,
    w_down,
):
    blocks = lax.axis_size(TP)
    groups = lax.axis_size(EP)
    rows, lanes = resid.shape
    heads = mix_gain.shape[0]
    items = groups * CAP
    bf16 = jnp.bfloat16
    shape = jax.ShapeDtypeStruct
    slots = groups * SLOTS
    new = shape((rows, heads), bf16)
    small = (
        resid,
        lengths.reshape(1, rows),
        attn_gain.reshape(blocks, lanes),
        mix_gain.reshape(1, heads),
        route_experts.T,
        route_weights.T,
    )
    near, *small = local(
        load_kernel,
        "load",
        [shape(x.shape, x.dtype) for x in small],
        *small,
        far_in=len(small),
        scratch=[pltpu.SemaphoreType.DMA((len(small),))],
    )
    copies = local(
        copies_kernel, "copies", shape((blocks, rows, lanes), bf16), near, flops=LONG
    )
    parts = exchange(copies, TP)
    new_keys, new_values, partial_branch, placed, high, low = local(
        attend_kernel,
        "attend",
        [new, new, shape((blocks, 3 * rows, lanes), bf16)] + [shape((slots, rows), bf16)] * 3,
        parts,
        *small,
        w_query.T,
        w_key.T,
        w_value.T,
        key_cache,
        value_cache,
        key_bias,
        w_out,
        far_out=2,
        scratch=[pltpu.VMEM((2, rows, heads), bf16), pltpu.SemaphoreType.DMA((2,))],
    )
    middle, outgoing = local(
        middle_kernel,
        "middle",
        [shape((rows, lanes), jnp.float32), shape((groups, 2 * SLOTS, lanes), bf16)],
        exchange(partial_branch, TP),
        parts,
        placed,
        flops=SHORT,
    )
    held = local(
        spread_kernel,
        "spread",
        shape((blocks // 2, 2 * items, lanes), bf16),
        exchange(outgoing, EP),
        flops=SHORT,
    )
    partial_out = local(
        expert_kernel,
        "expert",
        shape((blocks, items, lanes), bf16),
        exchange(held, NEAR),
        ffn_gain.reshape(blocks, lanes),
        w_gate,
        w_up,
        w_down,
    )
    result = local(
        total_kernel,
        "total",
        shape((groups, SLOTS, lanes), bf16),
        exchange(partial_out, TP),
        flops=SHORT,
    )
    mixed = local(
        mixture_kernel,
        "mixture",
        shape((rows, lanes), bf16),
        exchange(result, EP),
        middle,
        high,
        low,
    )
    return (mixed, new_keys, new_values)


def solution(mesh):
    torus = Mesh(
        mesh.devices.reshape(mesh.shape["ep"] // CORES, CORES, 4, 2, 2),
        ("ep_0", "ep_1", "tp_0", "tp_1", "tp_2"),
    )
    rows = ("ep_0", "ep_1")
    in_specs = (
        P(rows, TP),
        P(),
        P(None, TP),
        P(None, TP),
        P(None, TP),
        P(rows, TP, None, None),
        P(rows, TP, None, None),
        P(rows, TP, None),
        P(rows),
        P(TP),
        P(TP, None),
        P(),
        P(rows, None),
        P(rows, None),
        P(rows, None, TP),
        P(rows, None, TP),
        P(rows, TP, None),
    )
    out_specs = (P(rows, TP), P(rows, TP), P(rows, TP))
    return jax.shard_map(body, mesh=torus, in_specs=in_specs, out_specs=out_specs, check_vma=False)
```

```python
import jax
import jax.numpy as jnp
from jax import lax
from jax.experimental import pallas as pl
from jax.experimental.pallas import tpu as pltpu
from jax.sharding import Mesh
from jax.sharding import PartitionSpec as P


TP = ("tp_0", "tp_1")
EP = ("ep_1", "ep_0")
CORES = 2
PAIRS = (1, 4)

eps = 1e-06
limit = 7.0
alpha = 1.702
SLOTS = 4
CAP = 3
LIMIT = 16 * 1024 * 1024
LONG = 4 * 10**10
SHORT = 10**9


def project(rows, weight_ref):
    return lax.dot_general(
        rows, weight_ref[...], (((1,), (1,)), ((), ())), preferred_element_type=jnp.float32
    ).astype(jnp.bfloat16)


def chosen_slots(experts_ref, slots):
    top, rows = experts_ref.shape
    slot = lax.broadcasted_iota(jnp.int32, (slots, rows), 0)
    block = slot // SLOTS
    chips = slots // SLOTS // CORES
    expert = block % chips * CORES + block // chips
    hits = [experts_ref[k : k + 1, :] == expert for k in range(top)]
    named = hits[0]
    for hit in hits[1:]:
        named = named | hit
    first = lax.broadcasted_iota(jnp.int32, (rows, rows), 0)
    second = lax.broadcasted_iota(jnp.int32, (rows, rows), 1)
    earlier = (first < second).astype(jnp.bfloat16)
    rank = jnp.dot(
        named.astype(jnp.bfloat16), earlier, preferred_element_type=jnp.float32
    ).astype(jnp.int32)
    return hits, named & (rank == slot % SLOTS)


def attend_kernel(parts_ref, lengths_ref, gain_ref, mix_ref, experts_ref, share_ref, wq_ref,
                  wk_ref, wv_ref, key_ref, value_ref, bias_ref, wout_ref, new_key_ref,
                  new_value_ref, out_ref, placed_ref, high_ref, low_ref, fresh_ref, sems):
    blocks, rows, lanes = parts_ref.shape
    heads = key_ref.shape[2]
    cache = key_ref.shape[3]
    xs = [parts_ref[t].astype(jnp.float32) for t in range(blocks)]
    total = xs[0] * xs[0]
    for x in xs[1:]:
        total = total + x * x
    width = blocks * lanes
    scale = lax.rsqrt(jnp.sum(total, axis=1, keepdims=True) / width + eps)
    normed = jnp.concatenate(
        [(xs[t] * scale * gain_ref[t : t + 1, :]).astype(jnp.bfloat16) for t in range(blocks)],
        axis=1,
    )
    query = project(normed, wq_ref).astype(jnp.float32)
    fresh_ref[0] = project(normed, wk_ref)
    fresh_ref[1] = project(normed, wv_ref)
    stores = [
        pltpu.make_async_copy(fresh_ref.at[i], new_ref, sems.at[i])
        for i, new_ref in enumerate((new_key_ref, new_value_ref))
    ]
    for store in stores:
        store.start()
    spread = jnp.concatenate([query] * rows, axis=1)
    row = lax.broadcasted_iota(jnp.int32, spread.shape, 0)
    own = lax.broadcasted_iota(jnp.int32, spread.shape, 1) // heads == row
    spread = jnp.where(own, spread, 0.0).astype(jnp.bfloat16)
    keys = key_ref[:, 0].reshape(rows * heads, cache)
    scores = jnp.dot(spread, keys, preferred_element_type=jnp.float32) * heads ** (-0.5)
    scores = scores + bias_ref[:, 0, :]
    diagonal = lax.broadcasted_iota(jnp.int32, (rows, rows), 0) == lax.broadcasted_iota(
        jnp.int32, (rows, rows), 1
    )
    counts = lengths_ref[...].astype(jnp.float32)
    length = jnp.sum(jnp.where(diagonal, counts, 0.0), axis=1, keepdims=True).astype(jnp.int32)
    live = lax.broadcasted_iota(jnp.int32, (rows, cache), 1) < length
    soft = jnp.maximum(scores, 0.0) + jnp.log1p(jnp.exp(-jnp.abs(scores)))
    drop = jnp.where(live, soft, 0.0)
    chunks = cache // lanes
    stacked = jnp.concatenate([drop[:, c * lanes : (c + 1) * lanes] for c in range(chunks)], axis=0)
    below = lax.broadcasted_iota(jnp.int32, (lanes, lanes), 0)
    across = lax.broadcasted_iota(jnp.int32, (lanes, lanes), 1)
    later = (below > across).astype(jnp.bfloat16)
    high = stacked.astype(jnp.bfloat16)
    rest = stacked - high.astype(jnp.float32)
    middle = rest.astype(jnp.bfloat16)
    low = (rest - middle.astype(jnp.float32)).astype(jnp.bfloat16)
    after = (
        jnp.dot(high, later, preferred_element_type=jnp.float32)
        + jnp.dot(middle, later, preferred_element_type=jnp.float32)
        + jnp.dot(low, later, preferred_element_type=jnp.float32)
    )
    sums = jnp.sum(stacked, axis=1, keepdims=True)
    running = jnp.zeros((rows, 1), jnp.float32)
    pieces = [None] * chunks
    for c in reversed(range(chunks)):
        pieces[c] = after[c * rows : (c + 1) * rows] + running
        running = running + sums[c * rows : (c + 1) * rows]
    after = jnp.concatenate(pieces, axis=1)
    weights = jnp.where(live, jnp.exp(scores - soft - after), 0.0).astype(jnp.bfloat16)
    values = value_ref[:, 0].reshape(rows * heads, cache)
    crossed = lax.dot_general(
        weights, values, (((1,), (1,)), ((), ())), preferred_element_type=jnp.float32
    )
    crossed = jnp.where(own, crossed, 0.0)
    folded = crossed[:, :lanes]
    for c in range(1, crossed.shape[1] // lanes):
        folded = folded + crossed[:, c * lanes : (c + 1) * lanes]
    square = jnp.sum(folded * folded, axis=1, keepdims=True)
    attended = folded[:, :heads] + folded[:, heads : 2 * heads]
    ready = (attended * mix_ref[...]).astype(jnp.bfloat16)
    branch = jnp.dot(ready, wout_ref[...], preferred_element_type=jnp.float32)
    top = square.astype(jnp.bfloat16).astype(jnp.float32)
    half = lax.broadcasted_iota(jnp.int32, (rows, lanes), 1) < lanes // 2
    tail = jnp.where(half, top, square - top)
    for t in range(blocks):
        both = jnp.concatenate([branch[:, t * lanes : (t + 1) * lanes], tail], axis=0)
        out_ref[t] = both.astype(jnp.bfloat16)
    hits, placed = chosen_slots(experts_ref, placed_ref.shape[0])
    share = share_ref[...]
    share = share / jnp.sum(share, axis=0, keepdims=True)
    weight = jnp.where(hits[0], share[:1, :], 0.0)
    for k in range(1, len(hits)):
        weight = weight + jnp.where(hits[k], share[k : k + 1, :], 0.0)
    weight = jnp.where(placed, weight, 0.0)
    high = weight.astype(jnp.bfloat16)
    placed_ref[...] = placed.astype(jnp.bfloat16)
    high_ref[...] = high
    low_ref[...] = (weight - high.astype(jnp.float32)).astype(jnp.bfloat16)
    for store in stores:
        store.wait()


def load_kernel(*refs):
    count = len(refs) // 2
    sources, targets, sems = refs[:count], refs[count : 2 * count], refs[2 * count]
    loads = [
        pltpu.make_async_copy(source, target, sems.at[i])
        for i, (source, target) in enumerate(zip(sources, targets))
    ]
    for load in loads:
        load.start()
    for load in loads:
        load.wait()


def copies_kernel(row_ref, out_ref):
    row = row_ref[...]
    for t in range(out_ref.shape[0]):
        out_ref[t] = row


def middle_kernel(parts_ref, resid_ref, placed_ref, middle_ref, out_ref):
    blocks, both, lanes = parts_ref.shape
    rows = both // 2
    total = parts_ref[0].astype(jnp.float32)
    for t in range(1, blocks):
        total = total + parts_ref[t].astype(jnp.float32)
    square = total[rows:, :1] + total[rows:, lanes - 1 :]
    channels = blocks * (lanes // 2)
    scale = lax.rsqrt(square / channels + eps)
    middle = resid_ref[...].astype(jnp.float32) + total[:rows] * scale
    middle_ref[...] = middle
    out = jnp.dot(
        placed_ref[...], middle.astype(jnp.bfloat16), preferred_element_type=jnp.float32
    )
    out_ref[...] = out.reshape(out_ref.shape).astype(jnp.bfloat16)


def packing(items, slots):
    item = lax.broadcasted_iota(jnp.int32, (items, slots), 0)
    slot = lax.broadcasted_iota(jnp.int32, (items, slots), 1)
    return (item // CAP * SLOTS + item % CAP == slot).astype(jnp.bfloat16)


def spread_kernel(arrived_ref, out_ref):
    blocks, half, lanes = out_ref.shape
    groups, slots, _ = arrived_ref.shape
    arrived = arrived_ref[...].astype(jnp.float32).reshape(groups * slots, lanes)
    held = jnp.dot(
        packing(2 * half, groups * slots),
        arrived.astype(jnp.bfloat16),
        preferred_element_type=jnp.float32,
    ).astype(jnp.bfloat16)
    first = lax.axis_index(EP[0]) == 0
    halves = [held[i * half : (i + 1) * half] for i in range(2)]
    mixed = [jnp.where(first, halves[i], halves[1 - i]) for i in range(2)]
    for t in range(blocks):
        side, other = [int(t & step > 0) for step in PAIRS]
        out_ref[t] = halves[side] if side == other else mixed[side]


def total_kernel(parts_ref, out_ref):
    blocks, half, lanes = parts_ref.shape
    groups, slots, _ = out_ref.shape
    sums = {}
    for t in range(blocks):
        kind = tuple(int(t & step > 0) for step in PAIRS)
        part = parts_ref[t].astype(jnp.float32)
        sums[kind] = sums[kind] + part if kind in sums else part
    first = lax.axis_index(EP[0]) == 0
    total = [
        sums[i, i] + jnp.where(first, sums[i, 1 - i], sums[1 - i, i]) for i in range(2)
    ]
    total = jnp.concatenate(total, axis=0)
    spaced = lax.dot_general(
        packing(2 * half, groups * slots),
        total.astype(jnp.bfloat16),
        (((0,), (0,)), ((), ())),
        preferred_element_type=jnp.float32,
    )
    out_ref[...] = spaced.reshape(groups, slots, lanes).astype(jnp.bfloat16)


def mixture_kernel(returned_ref, middle_ref, high_ref, low_ref, out_ref):
    groups, slots, lanes = returned_ref.shape
    returned = returned_ref[...].astype(jnp.float32).reshape(groups * slots, lanes)
    returned = returned.astype(jnp.bfloat16)
    mixture = sum(
        lax.dot_general(
            part[...], returned, (((0,), (0,)), ((), ())), preferred_element_type=jnp.float32
        )
        for part in (high_ref, low_ref)
    )
    out_ref[...] = (middle_ref[...] + mixture).astype(jnp.bfloat16)


def expert_kernel(rows_ref, gain_ref, *refs):
    gates, ups, downs, out_ref = refs[0:2], refs[2:4], refs[4:6], refs[6]
    blocks, rows, lanes = rows_ref.shape
    total = jnp.zeros((rows, lanes), jnp.float32)
    scaled = []
    for t in range(blocks):
        x = rows_ref[t].astype(jnp.float32)
        total = total + x * x
        scaled.append((x * gain_ref[t : t + 1, :]).astype(jnp.bfloat16))
    scaled = jnp.concatenate(scaled, axis=1)
    scale = lax.rsqrt(jnp.sum(total, axis=1, keepdims=True) / (blocks * lanes) + eps)
    gate = jnp.concatenate([ref[0] for ref in gates], axis=1)
    gate = jnp.dot(scaled, gate, preferred_element_type=jnp.float32) * scale
    upper = jnp.concatenate([ref[0] for ref in ups], axis=1)
    upper = jnp.dot(scaled, upper, preferred_element_type=jnp.float32) * scale
    gate = jnp.minimum(gate, limit)
    upper = jnp.clip(upper, -limit, limit)
    active = ((upper + 1.0) * gate * jax.nn.sigmoid(alpha * gate)).astype(jnp.bfloat16)
    down = jnp.concatenate([ref[0] for ref in downs], axis=0)
    result = jnp.dot(active, down, preferred_element_type=jnp.float32).astype(jnp.bfloat16)
    for t in range(blocks):
        out_ref[t] = result[:, t * lanes : (t + 1) * lanes]


def local(kernel, out_shape, *args, flops=0, far_in=0, far_out=0, scratch=()):
    def places(count, far):
        return [pl.BlockSpec(memory_space=pltpu.HBM)] * far + [
            pl.BlockSpec(memory_space=pltpu.VMEM)
        ] * (count - far)

    single = not isinstance(out_shape, list)
    outs = places(1 if single else len(out_shape), far_out)
    return pl.pallas_call(
        kernel,
        in_specs=places(len(args), far_in),
        out_specs=outs[0] if single else outs,
        out_shape=out_shape,
        scratch_shapes=scratch,
        compiler_params=pltpu.CompilerParams(vmem_limit_bytes=LIMIT),
        cost_estimate=pl.CostEstimate(flops=flops, bytes_accessed=0, transcendentals=0),
    )(*[pltpu.with_memory_space_constraint(x, pltpu.HBM) for x in args[:far_in]], *args[far_in:])


def exchange(x, axis):
    return lax.all_to_all(x, axis, 0, 0, tiled=True)


def layer(
    resid,
    attn_gain,
    w_query,
    w_key,
    w_value,
    key_cache,
    value_cache,
    key_bias,
    lengths,
    mix_gain,
    w_out,
    ffn_gain,
    route_experts,
    route_weights,
    w_gate,
    w_up,
    w_down,
):
    blocks = lax.axis_size(TP)
    groups = lax.axis_size(EP)
    rows, lanes = resid.shape
    heads = mix_gain.shape[0]
    items = groups * CAP
    bf16 = jnp.bfloat16
    shape = jax.ShapeDtypeStruct
    slots = groups * SLOTS
    new = shape((rows, heads), bf16)
    small = (
        resid,
        lengths.reshape(1, rows),
        attn_gain.reshape(blocks, lanes),
        mix_gain.reshape(1, heads),
        route_experts.T,
        route_weights.T,
    )
    near, *small = local(
        load_kernel,
        [shape(x.shape, x.dtype) for x in small],
        *small,
        far_in=len(small),
        scratch=[pltpu.SemaphoreType.DMA((len(small),))],
    )
    copies = local(copies_kernel, shape((blocks, rows, lanes), bf16), near, flops=LONG)
    weights = []
    pairs = [(i, i ^ PAIRS[i // blocks]) for i in range(CORES * blocks)]
    for weight in (w_gate, w_up, w_down):
        weights += [weight, lax.ppermute(weight, (EP[0], *TP), pairs)]
    new_keys, new_values, partial_branch, placed, high, low = local(
        attend_kernel,
        [new, new, shape((blocks, 2 * rows, lanes), bf16)] + [shape((slots, rows), bf16)] * 3,
        exchange(copies, TP),
        *small,
        w_query.T,
        w_key.T,
        w_value.T,
        key_cache,
        value_cache,
        key_bias,
        w_out,
        far_out=2,
        scratch=[pltpu.VMEM((2, rows, heads), bf16), pltpu.SemaphoreType.DMA((2,))],
    )
    middle, outgoing = local(
        middle_kernel,
        [shape((rows, lanes), jnp.float32), shape((groups, SLOTS, lanes), bf16)],
        exchange(partial_branch, TP),
        near,
        placed,
        flops=SHORT,
    )
    arrived = exchange(outgoing, EP)
    held = local(spread_kernel, shape((blocks, items // 2, lanes), bf16), arrived, flops=SHORT)
    partial_out = local(
        expert_kernel,
        shape((blocks, items // 2, lanes), bf16),
        exchange(held, TP),
        ffn_gain.reshape(blocks, lanes),
        *weights,
    )
    result = local(
        total_kernel, shape((groups, SLOTS, lanes), bf16), exchange(partial_out, TP), flops=SHORT
    )
    mixed = local(
        mixture_kernel, shape((rows, lanes), bf16), exchange(result, EP), middle, high, low
    )
    return (mixed, new_keys, new_values)


def solution(mesh):
    torus = Mesh(
        mesh.devices.reshape(mesh.shape["ep"] // CORES, CORES, 4, 4),
        ("ep_0", "ep_1", "tp_0", "tp_1"),
    )
    rows = ("ep_0", "ep_1")
    in_specs = (
        P(rows, TP),
        P(),
        P(None, TP),
        P(None, TP),
        P(None, TP),
        P(rows, TP, None, None),
        P(rows, TP, None, None),
        P(rows, TP, None),
        P(rows),
        P(TP),
        P(TP, None),
        P(),
        P(rows, None),
        P(rows, None),
        P(rows, None, TP),
        P(rows, None, TP),
        P(rows, TP, None),
    )
    out_specs = (P(rows, TP), P(rows, TP), P(rows, TP))
    return jax.shard_map(layer, mesh=torus, in_specs=in_specs, out_specs=out_specs, check_vma=False)
```

```python
import jax
import jax.numpy as jnp
from jax import lax
from jax.experimental import pallas as pl
from jax.experimental.pallas import tpu as pltpu
from jax.sharding import Mesh
from jax.sharding import PartitionSpec as P


TP = ("tp_0", "tp_1")
EP = ("ep_1", "ep_0")
CORES = 2
PAIRS = (1, 4)

eps = 1e-06
limit = 7.0
alpha = 1.702
SLOTS = 4
CAP = 3
LIMIT = 16 * 1024 * 1024
LONG = 4 * 10**10
SHORT = 10**9


def project(rows, weight_ref):
    return lax.dot_general(
        rows, weight_ref[...], (((1,), (1,)), ((), ())), preferred_element_type=jnp.float32
    ).astype(jnp.bfloat16)


def chosen_slots(experts_ref, slots):
    top, rows = experts_ref.shape
    slot = lax.broadcasted_iota(jnp.int32, (slots, rows), 0)
    block = slot // SLOTS
    chips = slots // SLOTS // CORES
    expert = block % chips * CORES + block // chips
    hits = [experts_ref[k : k + 1, :] == expert for k in range(top)]
    named = hits[0]
    for hit in hits[1:]:
        named = named | hit
    first = lax.broadcasted_iota(jnp.int32, (rows, rows), 0)
    second = lax.broadcasted_iota(jnp.int32, (rows, rows), 1)
    earlier = (first < second).astype(jnp.bfloat16)
    rank = jnp.dot(
        named.astype(jnp.bfloat16), earlier, preferred_element_type=jnp.float32
    ).astype(jnp.int32)
    return hits, named & (rank == slot % SLOTS)


def attend_kernel(wgate_ref, wup_ref, wdown_ref, parts_ref, lengths_ref, gain_ref, mix_ref, experts_ref, share_ref, wq_ref,
                  wk_ref, wv_ref, key_ref, value_ref, bias_ref, wout_ref, new_key_ref,
                  new_value_ref, joined_ref, out_ref, placed_ref, high_ref, low_ref, fresh_ref,
                  sems, join_sems):
    blocks, rows, lanes = parts_ref.shape
    width = blocks * lanes
    pieces = [(wgate_ref.at[0], 0), (wup_ref.at[0], width)] + [
        (wdown_ref.at[0, :, pl.ds(t * lanes, lanes)], 2 * width + t * lanes) for t in range(blocks)
    ]
    joins = [
        pltpu.make_async_copy(
            source, joined_ref.at[pl.ds(start, source.shape[0])], join_sems.at[i]
        )
        for i, (source, start) in enumerate(pieces)
    ]
    for join in joins:
        join.start()
    heads = key_ref.shape[2]
    cache = key_ref.shape[3]
    xs = [parts_ref[t].astype(jnp.float32) for t in range(blocks)]
    total = xs[0] * xs[0]
    for x in xs[1:]:
        total = total + x * x
    scale = lax.rsqrt(jnp.sum(total, axis=1, keepdims=True) / width + eps)
    normed = jnp.concatenate(
        [(xs[t] * scale * gain_ref[t : t + 1, :]).astype(jnp.bfloat16) for t in range(blocks)],
        axis=1,
    )
    query = project(normed, wq_ref).astype(jnp.float32)
    fresh_ref[0] = project(normed, wk_ref)
    fresh_ref[1] = project(normed, wv_ref)
    stores = [
        pltpu.make_async_copy(fresh_ref.at[i], new_ref, sems.at[i])
        for i, new_ref in enumerate((new_key_ref, new_value_ref))
    ]
    for store in stores:
        store.start()
    spread = jnp.concatenate([query] * rows, axis=1)
    row = lax.broadcasted_iota(jnp.int32, spread.shape, 0)
    own = lax.broadcasted_iota(jnp.int32, spread.shape, 1) // heads == row
    spread = jnp.where(own, spread, 0.0).astype(jnp.bfloat16)
    keys = key_ref[:, 0].reshape(rows * heads, cache)
    scores = jnp.dot(spread, keys, preferred_element_type=jnp.float32) * heads ** (-0.5)
    scores = scores + bias_ref[:, 0, :]
    diagonal = lax.broadcasted_iota(jnp.int32, (rows, rows), 0) == lax.broadcasted_iota(
        jnp.int32, (rows, rows), 1
    )
    counts = lengths_ref[...].astype(jnp.float32)
    length = jnp.sum(jnp.where(diagonal, counts, 0.0), axis=1, keepdims=True).astype(jnp.int32)
    live = lax.broadcasted_iota(jnp.int32, (rows, cache), 1) < length
    soft = jnp.maximum(scores, 0.0) + jnp.log1p(jnp.exp(-jnp.abs(scores)))
    drop = jnp.where(live, soft, 0.0)
    chunks = cache // lanes
    stacked = jnp.concatenate([drop[:, c * lanes : (c + 1) * lanes] for c in range(chunks)], axis=0)
    below = lax.broadcasted_iota(jnp.int32, (lanes, lanes), 0)
    across = lax.broadcasted_iota(jnp.int32, (lanes, lanes), 1)
    later = (below > across).astype(jnp.bfloat16)
    high = stacked.astype(jnp.bfloat16)
    rest = stacked - high.astype(jnp.float32)
    middle = rest.astype(jnp.bfloat16)
    low = (rest - middle.astype(jnp.float32)).astype(jnp.bfloat16)
    after = (
        jnp.dot(high, later, preferred_element_type=jnp.float32)
        + jnp.dot(middle, later, preferred_element_type=jnp.float32)
        + jnp.dot(low, later, preferred_element_type=jnp.float32)
    )
    sums = jnp.sum(stacked, axis=1, keepdims=True)
    running = jnp.zeros((rows, 1), jnp.float32)
    pieces = [None] * chunks
    for c in reversed(range(chunks)):
        pieces[c] = after[c * rows : (c + 1) * rows] + running
        running = running + sums[c * rows : (c + 1) * rows]
    after = jnp.concatenate(pieces, axis=1)
    weights = jnp.where(live, jnp.exp(scores - soft - after), 0.0).astype(jnp.bfloat16)
    values = value_ref[:, 0].reshape(rows * heads, cache)
    crossed = lax.dot_general(
        weights, values, (((1,), (1,)), ((), ())), preferred_element_type=jnp.float32
    )
    crossed = jnp.where(own, crossed, 0.0)
    folded = crossed[:, :lanes]
    for c in range(1, crossed.shape[1] // lanes):
        folded = folded + crossed[:, c * lanes : (c + 1) * lanes]
    square = jnp.sum(folded * folded, axis=1, keepdims=True)
    attended = folded[:, :heads] + folded[:, heads : 2 * heads]
    ready = (attended * mix_ref[...]).astype(jnp.bfloat16)
    branch = jnp.dot(ready, wout_ref[...], preferred_element_type=jnp.float32)
    top = square.astype(jnp.bfloat16).astype(jnp.float32)
    half = lax.broadcasted_iota(jnp.int32, (rows, lanes), 1) < lanes // 2
    tail = jnp.where(half, top, square - top)
    for t in range(blocks):
        both = jnp.concatenate([branch[:, t * lanes : (t + 1) * lanes], tail], axis=0)
        out_ref[t] = both.astype(jnp.bfloat16)
    hits, placed = chosen_slots(experts_ref, placed_ref.shape[0])
    share = share_ref[...]
    share = share / jnp.sum(share, axis=0, keepdims=True)
    weight = jnp.where(hits[0], share[:1, :], 0.0)
    for k in range(1, len(hits)):
        weight = weight + jnp.where(hits[k], share[k : k + 1, :], 0.0)
    weight = jnp.where(placed, weight, 0.0)
    high = weight.astype(jnp.bfloat16)
    placed_ref[...] = placed.astype(jnp.bfloat16)
    high_ref[...] = high
    low_ref[...] = (weight - high.astype(jnp.float32)).astype(jnp.bfloat16)
    for copy in stores + joins:
        copy.wait()


def load_kernel(*refs):
    count = len(refs) // 2
    sources, targets, sems = refs[:count], refs[count : 2 * count], refs[2 * count]
    loads = [
        pltpu.make_async_copy(source, target, sems.at[i])
        for i, (source, target) in enumerate(zip(sources, targets))
    ]
    for load in loads:
        load.start()
    for load in loads:
        load.wait()


def copies_kernel(row_ref, out_ref):
    row = row_ref[...]
    for t in range(out_ref.shape[0]):
        out_ref[t] = row


def middle_kernel(parts_ref, resid_ref, placed_ref, middle_ref, out_ref):
    blocks, both, lanes = parts_ref.shape
    rows = both // 2
    total = parts_ref[0].astype(jnp.float32)
    for t in range(1, blocks):
        total = total + parts_ref[t].astype(jnp.float32)
    square = total[rows:, :1] + total[rows:, lanes - 1 :]
    channels = blocks * (lanes // 2)
    scale = lax.rsqrt(square / channels + eps)
    middle = resid_ref[...].astype(jnp.float32) + total[:rows] * scale
    middle_ref[...] = middle
    out = jnp.dot(
        placed_ref[...], middle.astype(jnp.bfloat16), preferred_element_type=jnp.float32
    )
    out_ref[...] = out.reshape(out_ref.shape).astype(jnp.bfloat16)


def packing(items, slots):
    item = lax.broadcasted_iota(jnp.int32, (items, slots), 0)
    slot = lax.broadcasted_iota(jnp.int32, (items, slots), 1)
    return (item // CAP * SLOTS + item % CAP == slot).astype(jnp.bfloat16)


def spread_kernel(arrived_ref, out_ref):
    blocks, half, lanes = out_ref.shape
    groups, slots, _ = arrived_ref.shape
    arrived = arrived_ref[...].astype(jnp.float32).reshape(groups * slots, lanes)
    held = jnp.dot(
        packing(2 * half, groups * slots),
        arrived.astype(jnp.bfloat16),
        preferred_element_type=jnp.float32,
    ).astype(jnp.bfloat16)
    first = lax.axis_index(EP[0]) == 0
    halves = [held[i * half : (i + 1) * half] for i in range(2)]
    mixed = [jnp.where(first, halves[i], halves[1 - i]) for i in range(2)]
    for t in range(blocks):
        side, other = [int(t & step > 0) for step in PAIRS]
        out_ref[t] = halves[side] if side == other else mixed[side]


def total_kernel(parts_ref, out_ref):
    blocks, half, lanes = parts_ref.shape
    groups, slots, _ = out_ref.shape
    sums = {}
    for t in range(blocks):
        kind = tuple(int(t & step > 0) for step in PAIRS)
        part = parts_ref[t].astype(jnp.float32)
        sums[kind] = sums[kind] + part if kind in sums else part
    first = lax.axis_index(EP[0]) == 0
    total = [
        sums[i, i] + jnp.where(first, sums[i, 1 - i], sums[1 - i, i]) for i in range(2)
    ]
    total = jnp.concatenate(total, axis=0)
    spaced = lax.dot_general(
        packing(2 * half, groups * slots),
        total.astype(jnp.bfloat16),
        (((0,), (0,)), ((), ())),
        preferred_element_type=jnp.float32,
    )
    out_ref[...] = spaced.reshape(groups, slots, lanes).astype(jnp.bfloat16)


def mixture_kernel(returned_ref, middle_ref, high_ref, low_ref, out_ref):
    groups, slots, lanes = returned_ref.shape
    returned = returned_ref[...].astype(jnp.float32).reshape(groups * slots, lanes)
    returned = returned.astype(jnp.bfloat16)
    mixture = sum(
        lax.dot_general(
            part[...], returned, (((0,), (0,)), ((), ())), preferred_element_type=jnp.float32
        )
        for part in (high_ref, low_ref)
    )
    out_ref[...] = (middle_ref[...] + mixture).astype(jnp.bfloat16)


def expert_kernel(rows_ref, gain_ref, *refs):
    gate_ref, up_ref, down_ref, joined_ref, out_ref = refs
    blocks, rows, lanes = rows_ref.shape
    total = jnp.zeros((rows, lanes), jnp.float32)
    scaled = []
    for t in range(blocks):
        x = rows_ref[t].astype(jnp.float32)
        total = total + x * x
        scaled.append((x * gain_ref[t : t + 1, :]).astype(jnp.bfloat16))
    scaled = jnp.concatenate(scaled, axis=1)
    scale = lax.rsqrt(jnp.sum(total, axis=1, keepdims=True) / (blocks * lanes) + eps)
    width = blocks * lanes
    gate = jnp.concatenate([gate_ref[0], joined_ref[:width]], axis=1)
    gate = jnp.dot(scaled, gate, preferred_element_type=jnp.float32) * scale
    upper = jnp.concatenate([up_ref[0], joined_ref[width : 2 * width]], axis=1)
    upper = jnp.dot(scaled, upper, preferred_element_type=jnp.float32) * scale
    gate = jnp.minimum(gate, limit)
    upper = jnp.clip(upper, -limit, limit)
    active = ((upper + 1.0) * gate * jax.nn.sigmoid(alpha * gate)).astype(jnp.bfloat16)
    other = [joined_ref[2 * width + t * lanes : 2 * width + (t + 1) * lanes] for t in range(blocks)]
    down = jnp.concatenate([down_ref[0], jnp.concatenate(other, axis=1)], axis=0)
    result = jnp.dot(active, down, preferred_element_type=jnp.float32).astype(jnp.bfloat16)
    for t in range(blocks):
        out_ref[t] = result[:, t * lanes : (t + 1) * lanes]


def local(kernel, out_shape, *args, flops=0, far_in=0, far_out=0, scratch=()):
    def places(count, far):
        return [pl.BlockSpec(memory_space=pltpu.HBM)] * far + [
            pl.BlockSpec(memory_space=pltpu.VMEM)
        ] * (count - far)

    single = not isinstance(out_shape, list)
    outs = places(1 if single else len(out_shape), far_out)
    return pl.pallas_call(
        kernel,
        in_specs=places(len(args), far_in),
        out_specs=outs[0] if single else outs,
        out_shape=out_shape,
        scratch_shapes=scratch,
        compiler_params=pltpu.CompilerParams(vmem_limit_bytes=LIMIT),
        cost_estimate=pl.CostEstimate(flops=flops, bytes_accessed=0, transcendentals=0),
    )(*[pltpu.with_memory_space_constraint(x, pltpu.HBM) for x in args[:far_in]], *args[far_in:])


def exchange(x, axis):
    return lax.all_to_all(x, axis, 0, 0, tiled=True)


def layer(
    resid,
    attn_gain,
    w_query,
    w_key,
    w_value,
    key_cache,
    value_cache,
    key_bias,
    lengths,
    mix_gain,
    w_out,
    ffn_gain,
    route_experts,
    route_weights,
    w_gate,
    w_up,
    w_down,
):
    blocks = lax.axis_size(TP)
    groups = lax.axis_size(EP)
    rows, lanes = resid.shape
    heads = mix_gain.shape[0]
    items = groups * CAP
    bf16 = jnp.bfloat16
    shape = jax.ShapeDtypeStruct
    slots = groups * SLOTS
    new = shape((rows, heads), bf16)
    small = (
        resid,
        lengths.reshape(1, rows),
        attn_gain.reshape(blocks, lanes),
        mix_gain.reshape(1, heads),
        route_experts.T,
        route_weights.T,
    )
    near, *small = local(
        load_kernel,
        [shape(x.shape, x.dtype) for x in small],
        *small,
        far_in=len(small),
        scratch=[pltpu.SemaphoreType.DMA((len(small),))],
    )
    copies = local(copies_kernel, shape((blocks, rows, lanes), bf16), near, flops=LONG)
    new_keys, new_values, joined, partial_branch, placed, high, low = local(
        attend_kernel,
        [new, new, shape((3 * blocks * lanes, lanes), bf16), shape((blocks, 2 * rows, lanes), bf16)]
        + [shape((slots, rows), bf16)] * 3,
        w_gate,
        w_up,
        w_down,
        exchange(copies, TP),
        *small,
        w_query.T,
        w_key.T,
        w_value.T,
        key_cache,
        value_cache,
        key_bias,
        w_out,
        far_in=3,
        far_out=3,
        scratch=[
            pltpu.VMEM((2, rows, heads), bf16),
            pltpu.SemaphoreType.DMA((2,)),
            pltpu.SemaphoreType.DMA((2 + blocks,)),
        ],
    )
    pairs = [(i, i ^ PAIRS[i // blocks]) for i in range(CORES * blocks)]
    branch = exchange(partial_branch, TP)
    joined = lax.ppermute(joined, (EP[0], *TP), pairs)
    middle, outgoing = local(
        middle_kernel,
        [shape((rows, lanes), jnp.float32), shape((groups, SLOTS, lanes), bf16)],
        branch,
        near,
        placed,
        flops=SHORT,
    )
    held = local(
        spread_kernel, shape((blocks, items // 2, lanes), bf16), exchange(outgoing, EP), flops=SHORT
    )
    partial_out = local(
        expert_kernel,
        shape((blocks, items // 2, lanes), bf16),
        exchange(held, TP),
        ffn_gain.reshape(blocks, lanes),
        w_gate,
        w_up,
        w_down,
        joined,
    )
    result = local(
        total_kernel, shape((groups, SLOTS, lanes), bf16), exchange(partial_out, TP), flops=SHORT
    )
    mixed = local(
        mixture_kernel, shape((rows, lanes), bf16), exchange(result, EP), middle, high, low
    )
    return (mixed, new_keys, new_values)


def solution(mesh):
    torus = Mesh(
        mesh.devices.reshape(mesh.shape["ep"] // CORES, CORES, 4, 4),
        ("ep_0", "ep_1", "tp_0", "tp_1"),
    )
    rows = ("ep_0", "ep_1")
    in_specs = (
        P(rows, TP),
        P(),
        P(None, TP),
        P(None, TP),
        P(None, TP),
        P(rows, TP, None, None),
        P(rows, TP, None, None),
        P(rows, TP, None),
        P(rows),
        P(TP),
        P(TP, None),
        P(),
        P(rows, None),
        P(rows, None),
        P(rows, None, TP),
        P(rows, None, TP),
        P(rows, TP, None),
    )
    out_specs = (P(rows, TP), P(rows, TP), P(rows, TP))
    return jax.shard_map(layer, mesh=torus, in_specs=in_specs, out_specs=out_specs, check_vma=False)
```

```python
import jax
import jax.numpy as jnp
from jax import lax
from jax.experimental import pallas as pl
from jax.experimental.pallas import tpu as pltpu
from jax.sharding import Mesh
from jax.sharding import PartitionSpec as P


TP = ("tp_0", "tp_1")
EP = ("ep_1", "ep_0")
CORES = 2
PAIRS = (1, 4)

eps = 1e-06
limit = 7.0
alpha = 1.702
SLOTS = 4
CAP = 3
LIMIT = 16 * 1024 * 1024
LONG = 4 * 10**10
SHORT = 10**9


def project(rows, weight_ref):
    return lax.dot_general(
        rows, weight_ref[...], (((1,), (1,)), ((), ())), preferred_element_type=jnp.float32
    ).astype(jnp.bfloat16)


def chosen_slots(experts_ref, slots):
    top, rows = experts_ref.shape
    slot = lax.broadcasted_iota(jnp.int32, (slots, rows), 0)
    block = slot // SLOTS
    chips = slots // SLOTS // CORES
    expert = block % chips * CORES + block // chips
    hits = [experts_ref[k : k + 1, :] == expert for k in range(top)]
    named = hits[0]
    for hit in hits[1:]:
        named = named | hit
    first = lax.broadcasted_iota(jnp.int32, (rows, rows), 0)
    second = lax.broadcasted_iota(jnp.int32, (rows, rows), 1)
    earlier = (first < second).astype(jnp.bfloat16)
    rank = jnp.dot(
        named.astype(jnp.bfloat16), earlier, preferred_element_type=jnp.float32
    ).astype(jnp.int32)
    return hits, named & (rank == slot % SLOTS)


def keys_kernel(normed_ref, wk_ref, wv_ref, new_key_ref, new_value_ref):
    new_key_ref[...] = project(normed_ref[...], wk_ref)
    new_value_ref[...] = project(normed_ref[...], wv_ref)


def attend_kernel(parts_ref, lengths_ref, gain_ref, mix_ref, experts_ref, share_ref, wq_ref,
                  key_ref, value_ref, bias_ref, wout_ref, normed_ref, out_ref, placed_ref,
                  high_ref, low_ref):
    blocks, rows, lanes = parts_ref.shape
    heads = key_ref.shape[2]
    cache = key_ref.shape[3]
    xs = [parts_ref[t].astype(jnp.float32) for t in range(blocks)]
    total = xs[0] * xs[0]
    for x in xs[1:]:
        total = total + x * x
    width = blocks * lanes
    scale = lax.rsqrt(jnp.sum(total, axis=1, keepdims=True) / width + eps)
    normed = jnp.concatenate(
        [(xs[t] * scale * gain_ref[t : t + 1, :]).astype(jnp.bfloat16) for t in range(blocks)],
        axis=1,
    )
    query = project(normed, wq_ref).astype(jnp.float32)
    normed_ref[...] = normed
    spread = jnp.concatenate([query] * rows, axis=1)
    row = lax.broadcasted_iota(jnp.int32, spread.shape, 0)
    own = lax.broadcasted_iota(jnp.int32, spread.shape, 1) // heads == row
    spread = jnp.where(own, spread, 0.0).astype(jnp.bfloat16)
    keys = key_ref[:, 0].reshape(rows * heads, cache)
    scores = jnp.dot(spread, keys, preferred_element_type=jnp.float32) * heads ** (-0.5)
    scores = scores + bias_ref[:, 0, :]
    diagonal = lax.broadcasted_iota(jnp.int32, (rows, rows), 0) == lax.broadcasted_iota(
        jnp.int32, (rows, rows), 1
    )
    counts = lengths_ref[...].astype(jnp.float32)
    length = jnp.sum(jnp.where(diagonal, counts, 0.0), axis=1, keepdims=True).astype(jnp.int32)
    live = lax.broadcasted_iota(jnp.int32, (rows, cache), 1) < length
    soft = jnp.maximum(scores, 0.0) + jnp.log1p(jnp.exp(-jnp.abs(scores)))
    drop = jnp.where(live, soft, 0.0)
    chunks = cache // lanes
    stacked = jnp.concatenate([drop[:, c * lanes : (c + 1) * lanes] for c in range(chunks)], axis=0)
    below = lax.broadcasted_iota(jnp.int32, (lanes, lanes), 0)
    across = lax.broadcasted_iota(jnp.int32, (lanes, lanes), 1)
    later = (below > across).astype(jnp.bfloat16)
    high = stacked.astype(jnp.bfloat16)
    rest = stacked - high.astype(jnp.float32)
    middle = rest.astype(jnp.bfloat16)
    low = (rest - middle.astype(jnp.float32)).astype(jnp.bfloat16)
    after = (
        jnp.dot(high, later, preferred_element_type=jnp.float32)
        + jnp.dot(middle, later, preferred_element_type=jnp.float32)
        + jnp.dot(low, later, preferred_element_type=jnp.float32)
    )
    sums = jnp.sum(stacked, axis=1, keepdims=True)
    running = jnp.zeros((rows, 1), jnp.float32)
    pieces = [None] * chunks
    for c in reversed(range(chunks)):
        pieces[c] = after[c * rows : (c + 1) * rows] + running
        running = running + sums[c * rows : (c + 1) * rows]
    after = jnp.concatenate(pieces, axis=1)
    weights = jnp.where(live, jnp.exp(scores - soft - after), 0.0).astype(jnp.bfloat16)
    values = value_ref[:, 0].reshape(rows * heads, cache)
    crossed = lax.dot_general(
        weights, values, (((1,), (1,)), ((), ())), preferred_element_type=jnp.float32
    )
    crossed = jnp.where(own, crossed, 0.0)
    folded = crossed[:, :lanes]
    for c in range(1, crossed.shape[1] // lanes):
        folded = folded + crossed[:, c * lanes : (c + 1) * lanes]
    square = jnp.sum(folded * folded, axis=1, keepdims=True)
    attended = folded[:, :heads] + folded[:, heads : 2 * heads]
    ready = (attended * mix_ref[...]).astype(jnp.bfloat16)
    branch = jnp.dot(ready, wout_ref[...], preferred_element_type=jnp.float32)
    top = square.astype(jnp.bfloat16).astype(jnp.float32)
    half = lax.broadcasted_iota(jnp.int32, (rows, lanes), 1) < lanes // 2
    tail = jnp.where(half, top, square - top)
    for t in range(blocks):
        both = jnp.concatenate([branch[:, t * lanes : (t + 1) * lanes], tail], axis=0)
        out_ref[t] = both.astype(jnp.bfloat16)
    hits, placed = chosen_slots(experts_ref, placed_ref.shape[0])
    share = share_ref[...]
    share = share / jnp.sum(share, axis=0, keepdims=True)
    weight = jnp.where(hits[0], share[:1, :], 0.0)
    for k in range(1, len(hits)):
        weight = weight + jnp.where(hits[k], share[k : k + 1, :], 0.0)
    weight = jnp.where(placed, weight, 0.0)
    high = weight.astype(jnp.bfloat16)
    placed_ref[...] = placed.astype(jnp.bfloat16)
    high_ref[...] = high
    low_ref[...] = (weight - high.astype(jnp.float32)).astype(jnp.bfloat16)


def load_kernel(*refs):
    count = len(refs) // 2
    sources, targets, sems = refs[:count], refs[count : 2 * count], refs[2 * count]
    loads = [
        pltpu.make_async_copy(source, target, sems.at[i])
        for i, (source, target) in enumerate(zip(sources, targets))
    ]
    for load in loads:
        load.start()
    for load in loads:
        load.wait()


def copies_kernel(row_ref, out_ref):
    row = row_ref[...]
    for t in range(out_ref.shape[0]):
        out_ref[t] = row


def join_kernel(gate_ref, up_ref, down_ref, after_ref, out_ref):
    lanes = out_ref.shape[1]
    width = gate_ref.shape[1]
    out_ref[:width] = gate_ref[0]
    out_ref[width : 2 * width] = up_ref[0]
    down = down_ref[0]
    for start in range(0, width, lanes):
        out_ref[2 * width + start : 2 * width + start + lanes] = down[:, start : start + lanes]


def middle_kernel(parts_ref, resid_ref, placed_ref, middle_ref, out_ref):
    blocks, both, lanes = parts_ref.shape
    rows = both // 2
    total = parts_ref[0].astype(jnp.float32)
    for t in range(1, blocks):
        total = total + parts_ref[t].astype(jnp.float32)
    square = total[rows:, :1] + total[rows:, lanes - 1 :]
    channels = blocks * (lanes // 2)
    scale = lax.rsqrt(square / channels + eps)
    middle = resid_ref[...].astype(jnp.float32) + total[:rows] * scale
    middle_ref[...] = middle
    out = jnp.dot(
        placed_ref[...], middle.astype(jnp.bfloat16), preferred_element_type=jnp.float32
    )
    out_ref[...] = out.reshape(out_ref.shape).astype(jnp.bfloat16)


def packing(items, slots):
    item = lax.broadcasted_iota(jnp.int32, (items, slots), 0)
    slot = lax.broadcasted_iota(jnp.int32, (items, slots), 1)
    return (item // CAP * SLOTS + item % CAP == slot).astype(jnp.bfloat16)


def spread_kernel(arrived_ref, out_ref):
    blocks, half, lanes = out_ref.shape
    groups, slots, _ = arrived_ref.shape
    arrived = arrived_ref[...].astype(jnp.float32).reshape(groups * slots, lanes)
    held = jnp.dot(
        packing(2 * half, groups * slots),
        arrived.astype(jnp.bfloat16),
        preferred_element_type=jnp.float32,
    ).astype(jnp.bfloat16)
    first = lax.axis_index(EP[0]) == 0
    halves = [held[i * half : (i + 1) * half] for i in range(2)]
    mixed = [jnp.where(first, halves[i], halves[1 - i]) for i in range(2)]
    for t in range(blocks):
        side, other = [int(t & step > 0) for step in PAIRS]
        out_ref[t] = halves[side] if side == other else mixed[side]


def total_kernel(parts_ref, out_ref):
    blocks, half, lanes = parts_ref.shape
    groups, slots, _ = out_ref.shape
    sums = {}
    for t in range(blocks):
        kind = tuple(int(t & step > 0) for step in PAIRS)
        part = parts_ref[t].astype(jnp.float32)
        sums[kind] = sums[kind] + part if kind in sums else part
    first = lax.axis_index(EP[0]) == 0
    total = [
        sums[i, i] + jnp.where(first, sums[i, 1 - i], sums[1 - i, i]) for i in range(2)
    ]
    total = jnp.concatenate(total, axis=0)
    spaced = lax.dot_general(
        packing(2 * half, groups * slots),
        total.astype(jnp.bfloat16),
        (((0,), (0,)), ((), ())),
        preferred_element_type=jnp.float32,
    )
    out_ref[...] = spaced.reshape(groups, slots, lanes).astype(jnp.bfloat16)


def mixture_kernel(returned_ref, middle_ref, high_ref, low_ref, out_ref):
    groups, slots, lanes = returned_ref.shape
    returned = returned_ref[...].astype(jnp.float32).reshape(groups * slots, lanes)
    returned = returned.astype(jnp.bfloat16)
    mixture = sum(
        lax.dot_general(
            part[...], returned, (((0,), (0,)), ((), ())), preferred_element_type=jnp.float32
        )
        for part in (high_ref, low_ref)
    )
    out_ref[...] = (middle_ref[...] + mixture).astype(jnp.bfloat16)


def expert_kernel(rows_ref, gain_ref, *refs):
    both, out_ref = refs[:2], refs[2]
    blocks, rows, lanes = rows_ref.shape
    total = jnp.zeros((rows, lanes), jnp.float32)
    scaled = []
    for t in range(blocks):
        x = rows_ref[t].astype(jnp.float32)
        total = total + x * x
        scaled.append((x * gain_ref[t : t + 1, :]).astype(jnp.bfloat16))
    scaled = jnp.concatenate(scaled, axis=1)
    scale = lax.rsqrt(jnp.sum(total, axis=1, keepdims=True) / (blocks * lanes) + eps)
    width = blocks * lanes
    gate = jnp.concatenate([ref[:width] for ref in both], axis=1)
    gate = jnp.dot(scaled, gate, preferred_element_type=jnp.float32) * scale
    upper = jnp.concatenate([ref[width : 2 * width] for ref in both], axis=1)
    upper = jnp.dot(scaled, upper, preferred_element_type=jnp.float32) * scale
    gate = jnp.minimum(gate, limit)
    upper = jnp.clip(upper, -limit, limit)
    active = ((upper + 1.0) * gate * jax.nn.sigmoid(alpha * gate)).astype(jnp.bfloat16)
    columns = [
        jnp.concatenate([ref[start : start + lanes] for ref in both], axis=0)
        for start in range(2 * width, 3 * width, lanes)
    ]
    down = jnp.concatenate(columns, axis=1)
    result = jnp.dot(active, down, preferred_element_type=jnp.float32).astype(jnp.bfloat16)
    for t in range(blocks):
        out_ref[t] = result[:, t * lanes : (t + 1) * lanes]


def local(kernel, out_shape, *args, flops=0, far_in=0, far_out=0, scratch=()):
    def places(count, far):
        return [pl.BlockSpec(memory_space=pltpu.HBM)] * far + [
            pl.BlockSpec(memory_space=pltpu.VMEM)
        ] * (count - far)

    single = not isinstance(out_shape, list)
    outs = places(1 if single else len(out_shape), far_out)
    return pl.pallas_call(
        kernel,
        in_specs=places(len(args), far_in),
        out_specs=outs[0] if single else outs,
        out_shape=out_shape,
        scratch_shapes=scratch,
        compiler_params=pltpu.CompilerParams(vmem_limit_bytes=LIMIT),
        cost_estimate=pl.CostEstimate(flops=flops, bytes_accessed=0, transcendentals=0),
    )(*[pltpu.with_memory_space_constraint(x, pltpu.HBM) for x in args[:far_in]], *args[far_in:])


def exchange(x, axis):
    return lax.all_to_all(x, axis, 0, 0, tiled=True)


def layer(
    resid,
    attn_gain,
    w_query,
    w_key,
    w_value,
    key_cache,
    value_cache,
    key_bias,
    lengths,
    mix_gain,
    w_out,
    ffn_gain,
    route_experts,
    route_weights,
    w_gate,
    w_up,
    w_down,
):
    blocks = lax.axis_size(TP)
    groups = lax.axis_size(EP)
    rows, lanes = resid.shape
    heads = mix_gain.shape[0]
    items = groups * CAP
    bf16 = jnp.bfloat16
    shape = jax.ShapeDtypeStruct
    slots = groups * SLOTS
    new = shape((rows, heads), bf16)
    small = (
        resid,
        lengths.reshape(1, rows),
        attn_gain.reshape(blocks, lanes),
        mix_gain.reshape(1, heads),
        route_experts.T,
        route_weights.T,
    )
    near, *small = local(
        load_kernel,
        [shape(x.shape, x.dtype) for x in small],
        *small,
        far_in=len(small),
        scratch=[pltpu.SemaphoreType.DMA((len(small),))],
    )
    copies = local(copies_kernel, shape((blocks, rows, lanes), bf16), near, flops=LONG)
    normed, partial_branch, placed, high, low = local(
        attend_kernel,
        [shape((rows, blocks * lanes), bf16), shape((blocks, 2 * rows, lanes), bf16)]
        + [shape((slots, rows), bf16)] * 3,
        exchange(copies, TP),
        *small,
        w_query.T,
        key_cache,
        value_cache,
        key_bias,
        w_out,
    )
    new_keys, new_values = local(keys_kernel, [new, new], normed, w_key.T, w_value.T, flops=SHORT)
    pairs = [(i, i ^ PAIRS[i // blocks]) for i in range(CORES * blocks)]
    branch = exchange(partial_branch, TP)
    joined = local(
        join_kernel,
        shape((3 * blocks * lanes, lanes), bf16),
        w_gate,
        w_up,
        w_down,
        low,
        flops=SHORT,
    )
    swapped = lax.ppermute(joined, (EP[0], *TP), pairs)
    middle, outgoing = local(
        middle_kernel,
        [shape((rows, lanes), jnp.float32), shape((groups, SLOTS, lanes), bf16)],
        branch,
        near,
        placed,
        flops=SHORT,
    )
    held = local(
        spread_kernel, shape((blocks, items // 2, lanes), bf16), exchange(outgoing, EP), flops=SHORT
    )
    partial_out = local(
        expert_kernel,
        shape((blocks, items // 2, lanes), bf16),
        exchange(held, TP),
        ffn_gain.reshape(blocks, lanes),
        joined,
        swapped,
    )
    result = local(
        total_kernel, shape((groups, SLOTS, lanes), bf16), exchange(partial_out, TP), flops=SHORT
    )
    mixed = local(
        mixture_kernel, shape((rows, lanes), bf16), exchange(result, EP), middle, high, low
    )
    return (mixed, new_keys, new_values)


def solution(mesh):
    torus = Mesh(
        mesh.devices.reshape(mesh.shape["ep"] // CORES, CORES, 4, 4),
        ("ep_0", "ep_1", "tp_0", "tp_1"),
    )
    rows = ("ep_0", "ep_1")
    in_specs = (
        P(rows, TP),
        P(),
        P(None, TP),
        P(None, TP),
        P(None, TP),
        P(rows, TP, None, None),
        P(rows, TP, None, None),
        P(rows, TP, None),
        P(rows),
        P(TP),
        P(TP, None),
        P(),
        P(rows, None),
        P(rows, None),
        P(rows, None, TP),
        P(rows, None, TP),
        P(rows, TP, None),
    )
    out_specs = (P(rows, TP), P(rows, TP), P(rows, TP))
    return jax.shard_map(layer, mesh=torus, in_specs=in_specs, out_specs=out_specs, check_vma=False)
```

```python
import jax
import jax.numpy as jnp
from jax import lax
from jax.experimental import pallas as pl
from jax.experimental.pallas import tpu as pltpu
from jax.sharding import Mesh
from jax.sharding import PartitionSpec as P


TP = ("tp_0", "tp_1")
EP = ("ep_1", "ep_0")
CORES = 2
PAIRS = (1, 4)
PIECE = 4

eps = 1e-06
limit = 7.0
alpha = 1.702
SLOTS = 4
CAP = 3
LIMIT = 16 * 1024 * 1024
LONG = 4 * 10**10
SHORT = 10**9


def project(rows, weight_ref):
    return lax.dot_general(
        rows, weight_ref[...], (((1,), (1,)), ((), ())), preferred_element_type=jnp.float32
    ).astype(jnp.bfloat16)


def chosen_slots(experts_ref, slots):
    top, rows = experts_ref.shape
    slot = lax.broadcasted_iota(jnp.int32, (slots, rows), 0)
    block = slot // SLOTS
    chips = slots // SLOTS // CORES
    expert = block % chips * CORES + block // chips
    hits = [experts_ref[k : k + 1, :] == expert for k in range(top)]
    named = hits[0]
    for hit in hits[1:]:
        named = named | hit
    first = lax.broadcasted_iota(jnp.int32, (rows, rows), 0)
    second = lax.broadcasted_iota(jnp.int32, (rows, rows), 1)
    earlier = (first < second).astype(jnp.bfloat16)
    rank = jnp.dot(
        named.astype(jnp.bfloat16), earlier, preferred_element_type=jnp.float32
    ).astype(jnp.int32)
    return hits, named & (rank == slot % SLOTS)


def attend_kernel(parts_ref, lengths_ref, gain_ref, mix_ref, experts_ref, share_ref, wq_ref,
                  wk_ref, wv_ref, key_ref, value_ref, bias_ref, wout_ref, new_key_ref,
                  new_value_ref, out_ref, placed_ref, high_ref, low_ref, fresh_ref, stage_ref, sems):
    blocks, rows, lanes = parts_ref.shape
    heads = key_ref.shape[2]
    cache = key_ref.shape[3]
    xs = [parts_ref[t].astype(jnp.float32) for t in range(blocks)]
    total = xs[0] * xs[0]
    for x in xs[1:]:
        total = total + x * x
    width = blocks * lanes
    scale = lax.rsqrt(jnp.sum(total, axis=1, keepdims=True) / width + eps)
    normed = jnp.concatenate(
        [(xs[t] * scale * gain_ref[t : t + 1, :]).astype(jnp.bfloat16) for t in range(blocks)],
        axis=1,
    )
    query = project(normed, wq_ref).astype(jnp.float32)
    fresh_ref[0] = project(normed, wk_ref)
    fresh_ref[1] = project(normed, wv_ref)
    stores = [
        pltpu.make_async_copy(fresh_ref.at[i], new_ref, sems.at[i])
        for i, new_ref in enumerate((new_key_ref, new_value_ref))
    ]
    for store in stores:
        store.start()
    spread = jnp.concatenate([query] * rows, axis=1)
    row = lax.broadcasted_iota(jnp.int32, spread.shape, 0)
    own = lax.broadcasted_iota(jnp.int32, spread.shape, 1) // heads == row
    spread = jnp.where(own, spread, 0.0).astype(jnp.bfloat16)
    keys = key_ref[:, 0].reshape(rows * heads, cache)
    scores = jnp.dot(spread, keys, preferred_element_type=jnp.float32) * heads ** (-0.5)
    scores = scores + bias_ref[:, 0, :]
    diagonal = lax.broadcasted_iota(jnp.int32, (rows, rows), 0) == lax.broadcasted_iota(
        jnp.int32, (rows, rows), 1
    )
    counts = lengths_ref[...].astype(jnp.float32)
    length = jnp.sum(jnp.where(diagonal, counts, 0.0), axis=1, keepdims=True).astype(jnp.int32)
    live = lax.broadcasted_iota(jnp.int32, (rows, cache), 1) < length
    soft = jnp.maximum(scores, 0.0) + jnp.log1p(jnp.exp(-jnp.abs(scores)))
    drop = jnp.where(live, soft, 0.0)
    chunks = cache // lanes
    stacked = jnp.concatenate([drop[:, c * lanes : (c + 1) * lanes] for c in range(chunks)], axis=0)
    below = lax.broadcasted_iota(jnp.int32, (lanes, lanes), 0)
    across = lax.broadcasted_iota(jnp.int32, (lanes, lanes), 1)
    later = (below > across).astype(jnp.bfloat16)
    high = stacked.astype(jnp.bfloat16)
    rest = stacked - high.astype(jnp.float32)
    middle = rest.astype(jnp.bfloat16)
    low = (rest - middle.astype(jnp.float32)).astype(jnp.bfloat16)
    after = (
        jnp.dot(high, later, preferred_element_type=jnp.float32)
        + jnp.dot(middle, later, preferred_element_type=jnp.float32)
        + jnp.dot(low, later, preferred_element_type=jnp.float32)
    )
    sums = jnp.sum(stacked, axis=1, keepdims=True)
    running = jnp.zeros((rows, 1), jnp.float32)
    pieces = [None] * chunks
    for c in reversed(range(chunks)):
        pieces[c] = after[c * rows : (c + 1) * rows] + running
        running = running + sums[c * rows : (c + 1) * rows]
    after = jnp.concatenate(pieces, axis=1)
    weights = jnp.where(live, jnp.exp(scores - soft - after), 0.0).astype(jnp.bfloat16)
    values = value_ref[:, 0].reshape(rows * heads, cache)
    crossed = lax.dot_general(
        weights, values, (((1,), (1,)), ((), ())), preferred_element_type=jnp.float32
    )
    crossed = jnp.where(own, crossed, 0.0)
    folded = crossed[:, :lanes]
    for c in range(1, crossed.shape[1] // lanes):
        folded = folded + crossed[:, c * lanes : (c + 1) * lanes]
    square = jnp.sum(folded * folded, axis=1, keepdims=True)
    attended = folded[:, :heads] + folded[:, heads : 2 * heads]
    ready = (attended * mix_ref[...]).astype(jnp.bfloat16)
    top = square.astype(jnp.bfloat16).astype(jnp.float32)
    half = lax.broadcasted_iota(jnp.int32, (rows, lanes), 1) < lanes // 2
    tail = jnp.where(half, top, square - top)
    tail = tail.astype(jnp.bfloat16)
    for t in range(blocks):
        stage_ref[t, rows:] = tail

    def send(first, last, low, high):
        store = pltpu.make_async_copy(
            stage_ref.at[first:last, low:high], out_ref.at[first:last, low:high], sems.at[len(stores)]
        )
        store.start()
        stores.append(store)

    send(0, blocks, rows, 2 * rows)
    branch = jnp.dot(ready, wout_ref[...], preferred_element_type=jnp.float32)
    for t in range(blocks):
        stage_ref[t, :rows] = branch[:, t * lanes : (t + 1) * lanes].astype(jnp.bfloat16)
        if t % PIECE == PIECE - 1:
            send(t + 1 - PIECE, t + 1, 0, rows)
    hits, placed = chosen_slots(experts_ref, placed_ref.shape[0])
    share = share_ref[...]
    share = share / jnp.sum(share, axis=0, keepdims=True)
    weight = jnp.where(hits[0], share[:1, :], 0.0)
    for k in range(1, len(hits)):
        weight = weight + jnp.where(hits[k], share[k : k + 1, :], 0.0)
    weight = jnp.where(placed, weight, 0.0)
    high = weight.astype(jnp.bfloat16)
    placed_ref[...] = placed.astype(jnp.bfloat16)
    high_ref[...] = high
    low_ref[...] = (weight - high.astype(jnp.float32)).astype(jnp.bfloat16)
    for store in stores:
        store.wait()


def load_kernel(*refs):
    count = len(refs) // 2
    sources, targets, sems = refs[:count], refs[count : 2 * count], refs[2 * count]
    loads = [
        pltpu.make_async_copy(source, target, sems.at[i])
        for i, (source, target) in enumerate(zip(sources, targets))
    ]
    for load in loads:
        load.start()
    for load in loads:
        load.wait()


def copies_kernel(row_ref, out_ref):
    row = row_ref[...]
    for t in range(out_ref.shape[0]):
        out_ref[t] = row


def join_kernel(gate_ref, up_ref, down_ref, after_ref, out_ref):
    lanes = out_ref.shape[1]
    width = gate_ref.shape[1]
    out_ref[:width] = gate_ref[0]
    out_ref[width : 2 * width] = up_ref[0]
    down = down_ref[0]
    for start in range(0, width, lanes):
        out_ref[2 * width + start : 2 * width + start + lanes] = down[:, start : start + lanes]


def middle_kernel(parts_ref, resid_ref, placed_ref, middle_ref, out_ref):
    blocks, both, lanes = parts_ref.shape
    rows = both // 2
    total = parts_ref[0].astype(jnp.float32)
    for t in range(1, blocks):
        total = total + parts_ref[t].astype(jnp.float32)
    square = total[rows:, :1] + total[rows:, lanes - 1 :]
    channels = blocks * (lanes // 2)
    scale = lax.rsqrt(square / channels + eps)
    middle = resid_ref[...].astype(jnp.float32) + total[:rows] * scale
    middle_ref[...] = middle
    out = jnp.dot(
        placed_ref[...], middle.astype(jnp.bfloat16), preferred_element_type=jnp.float32
    )
    out_ref[...] = out.reshape(out_ref.shape).astype(jnp.bfloat16)


def packing(items, slots):
    item = lax.broadcasted_iota(jnp.int32, (items, slots), 0)
    slot = lax.broadcasted_iota(jnp.int32, (items, slots), 1)
    return (item // CAP * SLOTS + item % CAP == slot).astype(jnp.bfloat16)


def spread_kernel(arrived_ref, out_ref):
    blocks, half, lanes = out_ref.shape
    groups, slots, _ = arrived_ref.shape
    arrived = arrived_ref[...].astype(jnp.float32).reshape(groups * slots, lanes)
    held = jnp.dot(
        packing(2 * half, groups * slots),
        arrived.astype(jnp.bfloat16),
        preferred_element_type=jnp.float32,
    ).astype(jnp.bfloat16)
    first = lax.axis_index(EP[0]) == 0
    halves = [held[i * half : (i + 1) * half] for i in range(2)]
    mixed = [jnp.where(first, halves[i], halves[1 - i]) for i in range(2)]
    for t in range(blocks):
        side, other = [int(t & step > 0) for step in PAIRS]
        out_ref[t] = halves[side] if side == other else mixed[side]


def total_kernel(parts_ref, out_ref):
    blocks, half, lanes = parts_ref.shape
    groups, slots, _ = out_ref.shape
    sums = {}
    for t in range(blocks):
        kind = tuple(int(t & step > 0) for step in PAIRS)
        part = parts_ref[t].astype(jnp.float32)
        sums[kind] = sums[kind] + part if kind in sums else part
    first = lax.axis_index(EP[0]) == 0
    total = [
        sums[i, i] + jnp.where(first, sums[i, 1 - i], sums[1 - i, i]) for i in range(2)
    ]
    total = jnp.concatenate(total, axis=0)
    spaced = lax.dot_general(
        packing(2 * half, groups * slots),
        total.astype(jnp.bfloat16),
        (((0,), (0,)), ((), ())),
        preferred_element_type=jnp.float32,
    )
    out_ref[...] = spaced.reshape(groups, slots, lanes).astype(jnp.bfloat16)


def mixture_kernel(returned_ref, middle_ref, high_ref, low_ref, out_ref):
    groups, slots, lanes = returned_ref.shape
    returned = returned_ref[...].astype(jnp.float32).reshape(groups * slots, lanes)
    returned = returned.astype(jnp.bfloat16)
    mixture = sum(
        lax.dot_general(
            part[...], returned, (((0,), (0,)), ((), ())), preferred_element_type=jnp.float32
        )
        for part in (high_ref, low_ref)
    )
    out_ref[...] = (middle_ref[...] + mixture).astype(jnp.bfloat16)


def expert_kernel(rows_ref, gain_ref, *refs):
    both, out_ref = refs[:2], refs[2]
    blocks, rows, lanes = rows_ref.shape
    total = jnp.zeros((rows, lanes), jnp.float32)
    scaled = []
    for t in range(blocks):
        x = rows_ref[t].astype(jnp.float32)
        total = total + x * x
        scaled.append((x * gain_ref[t : t + 1, :]).astype(jnp.bfloat16))
    scaled = jnp.concatenate(scaled, axis=1)
    scale = lax.rsqrt(jnp.sum(total, axis=1, keepdims=True) / (blocks * lanes) + eps)
    width = blocks * lanes
    gate = jnp.concatenate([ref[:width] for ref in both], axis=1)
    gate = jnp.dot(scaled, gate, preferred_element_type=jnp.float32) * scale
    upper = jnp.concatenate([ref[width : 2 * width] for ref in both], axis=1)
    upper = jnp.dot(scaled, upper, preferred_element_type=jnp.float32) * scale
    gate = jnp.minimum(gate, limit)
    upper = jnp.clip(upper, -limit, limit)
    active = ((upper + 1.0) * gate * jax.nn.sigmoid(alpha * gate)).astype(jnp.bfloat16)
    columns = [
        jnp.concatenate([ref[start : start + lanes] for ref in both], axis=0)
        for start in range(2 * width, 3 * width, lanes)
    ]
    down = jnp.concatenate(columns, axis=1)
    result = jnp.dot(active, down, preferred_element_type=jnp.float32).astype(jnp.bfloat16)
    for t in range(blocks):
        out_ref[t] = result[:, t * lanes : (t + 1) * lanes]


def local(kernel, out_shape, *args, flops=0, far_in=0, far_out=0, scratch=()):
    def places(count, far):
        return [pl.BlockSpec(memory_space=pltpu.HBM)] * far + [
            pl.BlockSpec(memory_space=pltpu.VMEM)
        ] * (count - far)

    single = not isinstance(out_shape, list)
    outs = places(1 if single else len(out_shape), far_out)
    return pl.pallas_call(
        kernel,
        in_specs=places(len(args), far_in),
        out_specs=outs[0] if single else outs,
        out_shape=out_shape,
        scratch_shapes=scratch,
        compiler_params=pltpu.CompilerParams(vmem_limit_bytes=LIMIT),
        cost_estimate=pl.CostEstimate(flops=flops, bytes_accessed=0, transcendentals=0),
    )(*[pltpu.with_memory_space_constraint(x, pltpu.HBM) for x in args[:far_in]], *args[far_in:])


def exchange(x, axis):
    return lax.all_to_all(x, axis, 0, 0, tiled=True)


def layer(
    resid,
    attn_gain,
    w_query,
    w_key,
    w_value,
    key_cache,
    value_cache,
    key_bias,
    lengths,
    mix_gain,
    w_out,
    ffn_gain,
    route_experts,
    route_weights,
    w_gate,
    w_up,
    w_down,
):
    blocks = lax.axis_size(TP)
    groups = lax.axis_size(EP)
    rows, lanes = resid.shape
    heads = mix_gain.shape[0]
    items = groups * CAP
    bf16 = jnp.bfloat16
    shape = jax.ShapeDtypeStruct
    slots = groups * SLOTS
    new = shape((rows, heads), bf16)
    small = (
        resid,
        lengths.reshape(1, rows),
        attn_gain.reshape(blocks, lanes),
        mix_gain.reshape(1, heads),
        route_experts.T,
        route_weights.T,
    )
    near, *small = local(
        load_kernel,
        [shape(x.shape, x.dtype) for x in small],
        *small,
        far_in=len(small),
        scratch=[pltpu.SemaphoreType.DMA((len(small),))],
    )
    copies = local(copies_kernel, shape((blocks, rows, lanes), bf16), near, flops=LONG)
    new_keys, new_values, partial_branch, placed, high, low = local(
        attend_kernel,
        [new, new, shape((blocks, 2 * rows, lanes), bf16)] + [shape((slots, rows), bf16)] * 3,
        exchange(copies, TP),
        *small,
        w_query.T,
        w_key.T,
        w_value.T,
        key_cache,
        value_cache,
        key_bias,
        w_out,
        far_out=3,
        scratch=[
            pltpu.VMEM((2, rows, heads), bf16),
            pltpu.VMEM((blocks, 2 * rows, lanes), bf16),
            pltpu.SemaphoreType.DMA((3 + blocks // PIECE,)),
        ],
    )
    pairs = [(i, i ^ PAIRS[i // blocks]) for i in range(CORES * blocks)]
    branch = exchange(partial_branch, TP)
    joined = local(
        join_kernel,
        shape((3 * blocks * lanes, lanes), bf16),
        w_gate,
        w_up,
        w_down,
        low,
        flops=SHORT,
    )
    swapped = lax.ppermute(joined, (EP[0], *TP), pairs)
    middle, outgoing = local(
        middle_kernel,
        [shape((rows, lanes), jnp.float32), shape((groups, SLOTS, lanes), bf16)],
        branch,
        near,
        placed,
        flops=SHORT,
    )
    held = local(
        spread_kernel, shape((blocks, items // 2, lanes), bf16), exchange(outgoing, EP), flops=SHORT
    )
    partial_out = local(
        expert_kernel,
        shape((blocks, items // 2, lanes), bf16),
        exchange(held, TP),
        ffn_gain.reshape(blocks, lanes),
        joined,
        swapped,
    )
    result = local(
        total_kernel, shape((groups, SLOTS, lanes), bf16), exchange(partial_out, TP), flops=SHORT
    )
    mixed = local(
        mixture_kernel, shape((rows, lanes), bf16), exchange(result, EP), middle, high, low
    )
    return (mixed, new_keys, new_values)


def solution(mesh):
    torus = Mesh(
        mesh.devices.reshape(mesh.shape["ep"] // CORES, CORES, 4, 4),
        ("ep_0", "ep_1", "tp_0", "tp_1"),
    )
    rows = ("ep_0", "ep_1")
    in_specs = (
        P(rows, TP),
        P(),
        P(None, TP),
        P(None, TP),
        P(None, TP),
        P(rows, TP, None, None),
        P(rows, TP, None, None),
        P(rows, TP, None),
        P(rows),
        P(TP),
        P(TP, None),
        P(),
        P(rows, None),
        P(rows, None),
        P(rows, None, TP),
        P(rows, None, TP),
        P(rows, TP, None),
    )
    out_specs = (P(rows, TP), P(rows, TP), P(rows, TP))
    return jax.shard_map(layer, mesh=torus, in_specs=in_specs, out_specs=out_specs, check_vma=False)
```

```python
import jax
import jax.numpy as jnp
from jax import lax
from jax.experimental import pallas as pl
from jax.experimental.pallas import tpu as pltpu
from jax.sharding import Mesh
from jax.sharding import PartitionSpec as P


TP = ("tp_0", "tp_1")
EP = ("ep_1", "ep_0")
CORES = 2
PAIRS = (1, 4)

eps = 1e-06
limit = 7.0
alpha = 1.702
SLOTS = 4
CAP = 3
LIMIT = 16 * 1024 * 1024
LONG = 4 * 10**10
SHORT = 10**9


def project(rows, weight_ref):
    return lax.dot_general(
        rows, weight_ref[...], (((1,), (1,)), ((), ())), preferred_element_type=jnp.float32
    ).astype(jnp.bfloat16)


def chosen_slots(experts_ref, slots):
    top, rows = experts_ref.shape
    slot = lax.broadcasted_iota(jnp.int32, (slots, rows), 0)
    block = slot // SLOTS
    chips = slots // SLOTS // CORES
    expert = block % chips * CORES + block // chips
    hits = [experts_ref[k : k + 1, :] == expert for k in range(top)]
    named = hits[0]
    for hit in hits[1:]:
        named = named | hit
    first = lax.broadcasted_iota(jnp.int32, (rows, rows), 0)
    second = lax.broadcasted_iota(jnp.int32, (rows, rows), 1)
    earlier = (first < second).astype(jnp.bfloat16)
    rank = jnp.dot(
        named.astype(jnp.bfloat16), earlier, preferred_element_type=jnp.float32
    ).astype(jnp.int32)
    return hits, named & (rank == slot % SLOTS)


def attend_kernel(far_key_ref, far_wk_ref, far_wv_ref, far_value_ref, far_wout_ref, parts_ref,
                  lengths_ref, gain_ref, mix_ref, experts_ref, share_ref, wq_ref, bias_ref,
                  new_key_ref, new_value_ref, out_ref, placed_ref, high_ref, low_ref, fresh_ref,
                  key_ref, wk_ref, wv_ref, value_ref, wout_ref, sems):
    far = (far_key_ref, far_wk_ref, far_wv_ref, far_value_ref, far_wout_ref)
    near = (key_ref, wk_ref, wv_ref, value_ref, wout_ref)
    fetches = [
        pltpu.make_async_copy(source, target, sems.at[2 + i])
        for i, (source, target) in enumerate(zip(far, near))
    ]
    for fetch in fetches:
        fetch.start()
    blocks, rows, lanes = parts_ref.shape
    heads = key_ref.shape[2]
    cache = key_ref.shape[3]
    xs = [parts_ref[t].astype(jnp.float32) for t in range(blocks)]
    total = xs[0] * xs[0]
    for x in xs[1:]:
        total = total + x * x
    width = blocks * lanes
    scale = lax.rsqrt(jnp.sum(total, axis=1, keepdims=True) / width + eps)
    normed = jnp.concatenate(
        [(xs[t] * scale * gain_ref[t : t + 1, :]).astype(jnp.bfloat16) for t in range(blocks)],
        axis=1,
    )
    query = project(normed, wq_ref).astype(jnp.float32)
    spread = jnp.concatenate([query] * rows, axis=1)
    row = lax.broadcasted_iota(jnp.int32, spread.shape, 0)
    own = lax.broadcasted_iota(jnp.int32, spread.shape, 1) // heads == row
    spread = jnp.where(own, spread, 0.0).astype(jnp.bfloat16)
    fetches[0].wait()
    keys = key_ref[:, 0].reshape(rows * heads, cache)
    scores = jnp.dot(spread, keys, preferred_element_type=jnp.float32) * heads ** (-0.5)
    scores = scores + bias_ref[:, 0, :]
    diagonal = lax.broadcasted_iota(jnp.int32, (rows, rows), 0) == lax.broadcasted_iota(
        jnp.int32, (rows, rows), 1
    )
    counts = lengths_ref[...].astype(jnp.float32)
    length = jnp.sum(jnp.where(diagonal, counts, 0.0), axis=1, keepdims=True).astype(jnp.int32)
    live = lax.broadcasted_iota(jnp.int32, (rows, cache), 1) < length
    fetches[1].wait()
    fetches[2].wait()
    fresh_ref[0] = project(normed, wk_ref)
    fresh_ref[1] = project(normed, wv_ref)
    stores = [
        pltpu.make_async_copy(fresh_ref.at[i], new_ref, sems.at[i])
        for i, new_ref in enumerate((new_key_ref, new_value_ref))
    ]
    for store in stores:
        store.start()
    soft = jnp.maximum(scores, 0.0) + jnp.log1p(jnp.exp(-jnp.abs(scores)))
    drop = jnp.where(live, soft, 0.0)
    chunks = cache // lanes
    stacked = jnp.concatenate([drop[:, c * lanes : (c + 1) * lanes] for c in range(chunks)], axis=0)
    below = lax.broadcasted_iota(jnp.int32, (lanes, lanes), 0)
    across = lax.broadcasted_iota(jnp.int32, (lanes, lanes), 1)
    later = (below > across).astype(jnp.bfloat16)
    high = stacked.astype(jnp.bfloat16)
    rest = stacked - high.astype(jnp.float32)
    middle = rest.astype(jnp.bfloat16)
    low = (rest - middle.astype(jnp.float32)).astype(jnp.bfloat16)
    after = (
        jnp.dot(high, later, preferred_element_type=jnp.float32)
        + jnp.dot(middle, later, preferred_element_type=jnp.float32)
        + jnp.dot(low, later, preferred_element_type=jnp.float32)
    )
    sums = jnp.sum(stacked, axis=1, keepdims=True)
    running = jnp.zeros((rows, 1), jnp.float32)
    pieces = [None] * chunks
    for c in reversed(range(chunks)):
        pieces[c] = after[c * rows : (c + 1) * rows] + running
        running = running + sums[c * rows : (c + 1) * rows]
    after = jnp.concatenate(pieces, axis=1)
    weights = jnp.where(live, jnp.exp(scores - soft - after), 0.0).astype(jnp.bfloat16)
    fetches[3].wait()
    values = value_ref[:, 0].reshape(rows * heads, cache)
    crossed = lax.dot_general(
        weights, values, (((1,), (1,)), ((), ())), preferred_element_type=jnp.float32
    )
    crossed = jnp.where(own, crossed, 0.0)
    folded = crossed[:, :lanes]
    for c in range(1, crossed.shape[1] // lanes):
        folded = folded + crossed[:, c * lanes : (c + 1) * lanes]
    square = jnp.sum(folded * folded, axis=1, keepdims=True)
    attended = folded[:, :heads] + folded[:, heads : 2 * heads]
    ready = (attended * mix_ref[...]).astype(jnp.bfloat16)
    fetches[4].wait()
    branch = jnp.dot(ready, wout_ref[...], preferred_element_type=jnp.float32)
    top = square.astype(jnp.bfloat16).astype(jnp.float32)
    half = lax.broadcasted_iota(jnp.int32, (rows, lanes), 1) < lanes // 2
    tail = jnp.where(half, top, square - top)
    for t in range(blocks):
        both = jnp.concatenate([branch[:, t * lanes : (t + 1) * lanes], tail], axis=0)
        out_ref[t] = both.astype(jnp.bfloat16)
    hits, placed = chosen_slots(experts_ref, placed_ref.shape[0])
    share = share_ref[...]
    share = share / jnp.sum(share, axis=0, keepdims=True)
    weight = jnp.where(hits[0], share[:1, :], 0.0)
    for k in range(1, len(hits)):
        weight = weight + jnp.where(hits[k], share[k : k + 1, :], 0.0)
    weight = jnp.where(placed, weight, 0.0)
    high = weight.astype(jnp.bfloat16)
    placed_ref[...] = placed.astype(jnp.bfloat16)
    high_ref[...] = high
    low_ref[...] = (weight - high.astype(jnp.float32)).astype(jnp.bfloat16)
    for store in stores:
        store.wait()


def load_kernel(*refs):
    count = len(refs) // 2 - 1
    sources, out_ref, targets, sems = refs[:count], refs[count], refs[count + 1 : -1], refs[-1]
    pairs = [(sources[0], out_ref.at[t]) for t in range(out_ref.shape[0])]
    pairs += list(zip(sources, targets))
    loads = [
        pltpu.make_async_copy(source, target, sems.at[i]) for i, (source, target) in enumerate(pairs)
    ]
    for load in loads:
        load.start()
    for load in loads:
        load.wait()


def join_kernel(gate_ref, up_ref, down_ref, after_ref, out_ref):
    lanes = out_ref.shape[1]
    width = gate_ref.shape[1]
    out_ref[:width] = gate_ref[0]
    out_ref[width : 2 * width] = up_ref[0]
    down = down_ref[0]
    for start in range(0, width, lanes):
        out_ref[2 * width + start : 2 * width + start + lanes] = down[:, start : start + lanes]


def middle_kernel(parts_ref, resid_ref, placed_ref, middle_ref, out_ref):
    blocks, both, lanes = parts_ref.shape
    rows = both // 2
    total = parts_ref[0].astype(jnp.float32)
    for t in range(1, blocks):
        total = total + parts_ref[t].astype(jnp.float32)
    square = total[rows:, :1] + total[rows:, lanes - 1 :]
    channels = blocks * (lanes // 2)
    scale = lax.rsqrt(square / channels + eps)
    middle = resid_ref[...].astype(jnp.float32) + total[:rows] * scale
    middle_ref[...] = middle
    out = jnp.dot(
        placed_ref[...], middle.astype(jnp.bfloat16), preferred_element_type=jnp.float32
    )
    out_ref[...] = out.reshape(out_ref.shape).astype(jnp.bfloat16)


def packing(items, slots):
    item = lax.broadcasted_iota(jnp.int32, (items, slots), 0)
    slot = lax.broadcasted_iota(jnp.int32, (items, slots), 1)
    return (item // CAP * SLOTS + item % CAP == slot).astype(jnp.bfloat16)


def spread_kernel(arrived_ref, out_ref):
    blocks, half, lanes = out_ref.shape
    groups, slots, _ = arrived_ref.shape
    arrived = arrived_ref[...].astype(jnp.float32).reshape(groups * slots, lanes)
    held = jnp.dot(
        packing(2 * half, groups * slots),
        arrived.astype(jnp.bfloat16),
        preferred_element_type=jnp.float32,
    ).astype(jnp.bfloat16)
    first = lax.axis_index(EP[0]) == 0
    halves = [held[i * half : (i + 1) * half] for i in range(2)]
    mixed = [jnp.where(first, halves[i], halves[1 - i]) for i in range(2)]
    for t in range(blocks):
        side, other = [int(t & step > 0) for step in PAIRS]
        out_ref[t] = halves[side] if side == other else mixed[side]


def total_kernel(parts_ref, out_ref):
    blocks, half, lanes = parts_ref.shape
    groups, slots, _ = out_ref.shape
    sums = {}
    for t in range(blocks):
        kind = tuple(int(t & step > 0) for step in PAIRS)
        part = parts_ref[t].astype(jnp.float32)
        sums[kind] = sums[kind] + part if kind in sums else part
    first = lax.axis_index(EP[0]) == 0
    total = [
        sums[i, i] + jnp.where(first, sums[i, 1 - i], sums[1 - i, i]) for i in range(2)
    ]
    total = jnp.concatenate(total, axis=0)
    spaced = lax.dot_general(
        packing(2 * half, groups * slots),
        total.astype(jnp.bfloat16),
        (((0,), (0,)), ((), ())),
        preferred_element_type=jnp.float32,
    )
    out_ref[...] = spaced.reshape(groups, slots, lanes).astype(jnp.bfloat16)


def mixture_kernel(returned_ref, middle_ref, high_ref, low_ref, out_ref):
    groups, slots, lanes = returned_ref.shape
    returned = returned_ref[...].astype(jnp.float32).reshape(groups * slots, lanes)
    returned = returned.astype(jnp.bfloat16)
    mixture = sum(
        lax.dot_general(
            part[...], returned, (((0,), (0,)), ((), ())), preferred_element_type=jnp.float32
        )
        for part in (high_ref, low_ref)
    )
    out_ref[...] = (middle_ref[...] + mixture).astype(jnp.bfloat16)


def expert_kernel(rows_ref, gain_ref, *refs):
    both, out_ref = refs[:2], refs[2]
    blocks, rows, lanes = rows_ref.shape
    total = jnp.zeros((rows, lanes), jnp.float32)
    scaled = []
    for t in range(blocks):
        x = rows_ref[t].astype(jnp.float32)
        total = total + x * x
        scaled.append((x * gain_ref[t : t + 1, :]).astype(jnp.bfloat16))
    scaled = jnp.concatenate(scaled, axis=1)
    scale = lax.rsqrt(jnp.sum(total, axis=1, keepdims=True) / (blocks * lanes) + eps)
    width = blocks * lanes
    gate = jnp.concatenate([ref[:width] for ref in both], axis=1)
    gate = jnp.dot(scaled, gate, preferred_element_type=jnp.float32) * scale
    upper = jnp.concatenate([ref[width : 2 * width] for ref in both], axis=1)
    upper = jnp.dot(scaled, upper, preferred_element_type=jnp.float32) * scale
    gate = jnp.minimum(gate, limit)
    upper = jnp.clip(upper, -limit, limit)
    active = ((upper + 1.0) * gate * jax.nn.sigmoid(alpha * gate)).astype(jnp.bfloat16)
    columns = [
        jnp.concatenate([ref[start : start + lanes] for ref in both], axis=0)
        for start in range(2 * width, 3 * width, lanes)
    ]
    down = jnp.concatenate(columns, axis=1)
    result = jnp.dot(active, down, preferred_element_type=jnp.float32).astype(jnp.bfloat16)
    for t in range(blocks):
        out_ref[t] = result[:, t * lanes : (t + 1) * lanes]


def local(kernel, out_shape, *args, flops=0, far_in=0, far_out=0, scratch=()):
    def places(count, far):
        return [pl.BlockSpec(memory_space=pltpu.HBM)] * far + [
            pl.BlockSpec(memory_space=pltpu.VMEM)
        ] * (count - far)

    single = not isinstance(out_shape, list)
    outs = places(1 if single else len(out_shape), far_out)
    return pl.pallas_call(
        kernel,
        in_specs=places(len(args), far_in),
        out_specs=outs[0] if single else outs,
        out_shape=out_shape,
        scratch_shapes=scratch,
        compiler_params=pltpu.CompilerParams(vmem_limit_bytes=LIMIT),
        cost_estimate=pl.CostEstimate(flops=flops, bytes_accessed=0, transcendentals=0),
    )(*[pltpu.with_memory_space_constraint(x, pltpu.HBM) for x in args[:far_in]], *args[far_in:])


def exchange(x, axis):
    return lax.all_to_all(x, axis, 0, 0, tiled=True)


def layer(
    resid,
    attn_gain,
    w_query,
    w_key,
    w_value,
    key_cache,
    value_cache,
    key_bias,
    lengths,
    mix_gain,
    w_out,
    ffn_gain,
    route_experts,
    route_weights,
    w_gate,
    w_up,
    w_down,
):
    blocks = lax.axis_size(TP)
    groups = lax.axis_size(EP)
    rows, lanes = resid.shape
    heads = mix_gain.shape[0]
    items = groups * CAP
    bf16 = jnp.bfloat16
    shape = jax.ShapeDtypeStruct
    slots = groups * SLOTS
    new = shape((rows, heads), bf16)
    small = (
        resid,
        lengths.reshape(1, rows),
        attn_gain.reshape(blocks, lanes),
        mix_gain.reshape(1, heads),
        route_experts.T,
        route_weights.T,
    )
    copies, near, *small = local(
        load_kernel,
        [shape((blocks, rows, lanes), bf16)] + [shape(x.shape, x.dtype) for x in small],
        *small,
        flops=LONG,
        far_in=len(small),
        far_out=1,
        scratch=[pltpu.SemaphoreType.DMA((blocks + len(small),))],
    )
    parts = exchange(copies, TP)
    new_keys, new_values, partial_branch, placed, high, low = local(
        attend_kernel,
        [new, new, shape((blocks, 2 * rows, lanes), bf16)] + [shape((slots, rows), bf16)] * 3,
        key_cache,
        w_key.T,
        w_value.T,
        value_cache,
        w_out,
        parts,
        *small,
        w_query.T,
        key_bias,
        far_in=5,
        far_out=2,
        scratch=[
            pltpu.VMEM((2, rows, heads), bf16),
            pltpu.VMEM(key_cache.shape, bf16),
            pltpu.VMEM(w_key.T.shape, bf16),
            pltpu.VMEM(w_value.T.shape, bf16),
            pltpu.VMEM(value_cache.shape, bf16),
            pltpu.VMEM(w_out.shape, bf16),
            pltpu.SemaphoreType.DMA((7,)),
        ],
    )
    pairs = [(i, i ^ PAIRS[i // blocks]) for i in range(CORES * blocks)]
    branch = exchange(partial_branch, TP)
    joined = local(
        join_kernel,
        shape((3 * blocks * lanes, lanes), bf16),
        w_gate,
        w_up,
        w_down,
        near,
        flops=SHORT,
    )
    swapped = lax.ppermute(joined, (EP[0], *TP), pairs)
    middle, outgoing = local(
        middle_kernel,
        [shape((rows, lanes), jnp.float32), shape((groups, SLOTS, lanes), bf16)],
        branch,
        near,
        placed,
        flops=SHORT,
    )
    held = local(
        spread_kernel, shape((blocks, items // 2, lanes), bf16), exchange(outgoing, EP), flops=SHORT
    )
    partial_out = local(
        expert_kernel,
        shape((blocks, items // 2, lanes), bf16),
        exchange(held, TP),
        ffn_gain.reshape(blocks, lanes),
        joined,
        swapped,
    )
    result = local(
        total_kernel, shape((groups, SLOTS, lanes), bf16), exchange(partial_out, TP), flops=SHORT
    )
    mixed = local(
        mixture_kernel, shape((rows, lanes), bf16), exchange(result, EP), middle, high, low
    )
    return (mixed, new_keys, new_values)


def solution(mesh):
    torus = Mesh(
        mesh.devices.reshape(mesh.shape["ep"] // CORES, CORES, 4, 4),
        ("ep_0", "ep_1", "tp_0", "tp_1"),
    )
    rows = ("ep_0", "ep_1")
    in_specs = (
        P(rows, TP),
        P(),
        P(None, TP),
        P(None, TP),
        P(None, TP),
        P(rows, TP, None, None),
        P(rows, TP, None, None),
        P(rows, TP, None),
        P(rows),
        P(TP),
        P(TP, None),
        P(),
        P(rows, None),
        P(rows, None),
        P(rows, None, TP),
        P(rows, None, TP),
        P(rows, TP, None),
    )
    out_specs = (P(rows, TP), P(rows, TP), P(rows, TP))
    return jax.shard_map(layer, mesh=torus, in_specs=in_specs, out_specs=out_specs, check_vma=False)
```

```python
import jax
import jax.numpy as jnp
from jax import lax
from jax.experimental import pallas as pl
from jax.experimental.pallas import tpu as pltpu
from jax.sharding import Mesh
from jax.sharding import PartitionSpec as P


TP = ("tp_0", "tp_1")
EP = ("ep_1", "ep_0")
CORES = 2
PAIRS = (4, 1)

eps = 1e-06
limit = 7.0
alpha = 1.702
SLOTS = 4
CAP = 3
LIMIT = 16 * 1024 * 1024
LONG = 4 * 10**10
SHORT = 10**9


def project(rows, weight_ref):
    return lax.dot_general(
        rows, weight_ref[...], (((1,), (1,)), ((), ())), preferred_element_type=jnp.float32
    ).astype(jnp.bfloat16)


def chosen_slots(experts_ref, slots):
    top, rows = experts_ref.shape
    slot = lax.broadcasted_iota(jnp.int32, (slots, rows), 0)
    block = slot // SLOTS
    chips = slots // SLOTS // CORES
    expert = block % chips * CORES + block // chips
    hits = [experts_ref[k : k + 1, :] == expert for k in range(top)]
    named = hits[0]
    for hit in hits[1:]:
        named = named | hit
    first = lax.broadcasted_iota(jnp.int32, (rows, rows), 0)
    second = lax.broadcasted_iota(jnp.int32, (rows, rows), 1)
    earlier = (first < second).astype(jnp.bfloat16)
    rank = jnp.dot(
        named.astype(jnp.bfloat16), earlier, preferred_element_type=jnp.float32
    ).astype(jnp.int32)
    return hits, named & (rank == slot % SLOTS)


def attend_kernel(parts_ref, lengths_ref, gain_ref, mix_ref, experts_ref, share_ref, wq_ref,
                  wk_ref, wv_ref, key_ref, value_ref, bias_ref, wout_ref, new_key_ref,
                  new_value_ref, out_ref, placed_ref, high_ref, low_ref, fresh_ref, sems):
    blocks, rows, lanes = parts_ref.shape
    heads = key_ref.shape[2]
    cache = key_ref.shape[3]
    xs = [parts_ref[t].astype(jnp.float32) for t in range(blocks)]
    total = xs[0] * xs[0]
    for x in xs[1:]:
        total = total + x * x
    width = blocks * lanes
    scale = lax.rsqrt(jnp.sum(total, axis=1, keepdims=True) / width + eps)
    normed = jnp.concatenate(
        [(xs[t] * scale * gain_ref[t : t + 1, :]).astype(jnp.bfloat16) for t in range(blocks)],
        axis=1,
    )
    query = project(normed, wq_ref).astype(jnp.float32)
    fresh_ref[0] = project(normed, wk_ref)
    fresh_ref[1] = project(normed, wv_ref)
    stores = [
        pltpu.make_async_copy(fresh_ref.at[i], new_ref, sems.at[i])
        for i, new_ref in enumerate((new_key_ref, new_value_ref))
    ]
    for store in stores:
        store.start()
    spread = jnp.concatenate([query] * rows, axis=1)
    row = lax.broadcasted_iota(jnp.int32, spread.shape, 0)
    own = lax.broadcasted_iota(jnp.int32, spread.shape, 1) // heads == row
    spread = jnp.where(own, spread, 0.0).astype(jnp.bfloat16)
    keys = key_ref[:, 0].reshape(rows * heads, cache)
    scores = jnp.dot(spread, keys, preferred_element_type=jnp.float32) * heads ** (-0.5)
    scores = scores + bias_ref[:, 0, :]
    diagonal = lax.broadcasted_iota(jnp.int32, (rows, rows), 0) == lax.broadcasted_iota(
        jnp.int32, (rows, rows), 1
    )
    counts = lengths_ref[...].astype(jnp.float32)
    length = jnp.sum(jnp.where(diagonal, counts, 0.0), axis=1, keepdims=True).astype(jnp.int32)
    live = lax.broadcasted_iota(jnp.int32, (rows, cache), 1) < length
    soft = jnp.maximum(scores, 0.0) + jnp.log1p(jnp.exp(-jnp.abs(scores)))
    drop = jnp.where(live, soft, 0.0)
    chunks = cache // lanes
    stacked = jnp.concatenate([drop[:, c * lanes : (c + 1) * lanes] for c in range(chunks)], axis=0)
    below = lax.broadcasted_iota(jnp.int32, (lanes, lanes), 0)
    across = lax.broadcasted_iota(jnp.int32, (lanes, lanes), 1)
    later = (below > across).astype(jnp.bfloat16)
    high = stacked.astype(jnp.bfloat16)
    rest = stacked - high.astype(jnp.float32)
    middle = rest.astype(jnp.bfloat16)
    low = (rest - middle.astype(jnp.float32)).astype(jnp.bfloat16)
    after = (
        jnp.dot(high, later, preferred_element_type=jnp.float32)
        + jnp.dot(middle, later, preferred_element_type=jnp.float32)
        + jnp.dot(low, later, preferred_element_type=jnp.float32)
    )
    sums = jnp.sum(stacked, axis=1, keepdims=True)
    running = jnp.zeros((rows, 1), jnp.float32)
    pieces = [None] * chunks
    for c in reversed(range(chunks)):
        pieces[c] = after[c * rows : (c + 1) * rows] + running
        running = running + sums[c * rows : (c + 1) * rows]
    after = jnp.concatenate(pieces, axis=1)
    weights = jnp.where(live, jnp.exp(scores - soft - after), 0.0).astype(jnp.bfloat16)
    values = value_ref[:, 0].reshape(rows * heads, cache)
    crossed = lax.dot_general(
        weights, values, (((1,), (1,)), ((), ())), preferred_element_type=jnp.float32
    )
    crossed = jnp.where(own, crossed, 0.0)
    folded = crossed[:, :lanes]
    for c in range(1, crossed.shape[1] // lanes):
        folded = folded + crossed[:, c * lanes : (c + 1) * lanes]
    square = jnp.sum(folded * folded, axis=1, keepdims=True)
    attended = folded[:, :heads] + folded[:, heads : 2 * heads]
    ready = (attended * mix_ref[...]).astype(jnp.bfloat16)
    branch = jnp.dot(ready, wout_ref[...], preferred_element_type=jnp.float32)
    top = square.astype(jnp.bfloat16).astype(jnp.float32)
    half = lax.broadcasted_iota(jnp.int32, (rows, lanes), 1) < lanes // 2
    tail = jnp.where(half, top, square - top)
    for t in range(blocks):
        both = jnp.concatenate([branch[:, t * lanes : (t + 1) * lanes], tail], axis=0)
        out_ref[t] = both.astype(jnp.bfloat16)
    hits, placed = chosen_slots(experts_ref, placed_ref.shape[0])
    share = share_ref[...]
    share = share / jnp.sum(share, axis=0, keepdims=True)
    weight = jnp.where(hits[0], share[:1, :], 0.0)
    for k in range(1, len(hits)):
        weight = weight + jnp.where(hits[k], share[k : k + 1, :], 0.0)
    weight = jnp.where(placed, weight, 0.0)
    high = weight.astype(jnp.bfloat16)
    placed_ref[...] = placed.astype(jnp.bfloat16)
    high_ref[...] = high
    low_ref[...] = (weight - high.astype(jnp.float32)).astype(jnp.bfloat16)
    for store in stores:
        store.wait()


def load_kernel(*refs):
    count = len(refs) // 2
    sources, targets, sems = refs[:count], refs[count : 2 * count], refs[2 * count]
    loads = [
        pltpu.make_async_copy(source, target, sems.at[i])
        for i, (source, target) in enumerate(zip(sources, targets))
    ]
    for load in loads:
        load.start()
    for load in loads:
        load.wait()


def copies_kernel(row_ref, out_ref):
    row = row_ref[...]
    for t in range(out_ref.shape[0]):
        out_ref[t] = row


def join_kernel(gate_ref, up_ref, down_ref, after_ref, out_ref):
    lanes = out_ref.shape[1]
    width = gate_ref.shape[1]
    out_ref[:width] = gate_ref[0]
    out_ref[width : 2 * width] = up_ref[0]
    down = down_ref[0]
    for start in range(0, width, lanes):
        out_ref[2 * width + start : 2 * width + start + lanes] = down[:, start : start + lanes]


def middle_kernel(parts_ref, resid_ref, placed_ref, middle_ref, out_ref):
    blocks, both, lanes = parts_ref.shape
    rows = both // 2
    total = parts_ref[0].astype(jnp.float32)
    for t in range(1, blocks):
        total = total + parts_ref[t].astype(jnp.float32)
    square = total[rows:, :1] + total[rows:, lanes - 1 :]
    channels = blocks * (lanes // 2)
    scale = lax.rsqrt(square / channels + eps)
    middle = resid_ref[...].astype(jnp.float32) + total[:rows] * scale
    middle_ref[...] = middle
    out = jnp.dot(
        placed_ref[...], middle.astype(jnp.bfloat16), preferred_element_type=jnp.float32
    )
    out_ref[...] = out.reshape(out_ref.shape).astype(jnp.bfloat16)


def packing(items, slots):
    item = lax.broadcasted_iota(jnp.int32, (items, slots), 0)
    slot = lax.broadcasted_iota(jnp.int32, (items, slots), 1)
    return (item // CAP * SLOTS + item % CAP == slot).astype(jnp.bfloat16)


def spread_kernel(arrived_ref, out_ref):
    blocks, half, lanes = out_ref.shape
    groups, slots, _ = arrived_ref.shape
    arrived = arrived_ref[...].astype(jnp.float32).reshape(groups * slots, lanes)
    held = jnp.dot(
        packing(2 * half, groups * slots),
        arrived.astype(jnp.bfloat16),
        preferred_element_type=jnp.float32,
    ).astype(jnp.bfloat16)
    first = lax.axis_index(EP[0]) == 0
    halves = [held[i * half : (i + 1) * half] for i in range(2)]
    mixed = [jnp.where(first, halves[i], halves[1 - i]) for i in range(2)]
    for t in range(blocks):
        side, other = [int(t & step > 0) for step in PAIRS]
        out_ref[t] = halves[side] if side == other else mixed[side]


def total_kernel(parts_ref, out_ref):
    blocks, half, lanes = parts_ref.shape
    groups, slots, _ = out_ref.shape
    sums = {}
    for t in range(blocks):
        kind = tuple(int(t & step > 0) for step in PAIRS)
        part = parts_ref[t].astype(jnp.float32)
        sums[kind] = sums[kind] + part if kind in sums else part
    first = lax.axis_index(EP[0]) == 0
    total = [
        sums[i, i] + jnp.where(first, sums[i, 1 - i], sums[1 - i, i]) for i in range(2)
    ]
    total = jnp.concatenate(total, axis=0)
    spaced = lax.dot_general(
        packing(2 * half, groups * slots),
        total.astype(jnp.bfloat16),
        (((0,), (0,)), ((), ())),
        preferred_element_type=jnp.float32,
    )
    out_ref[...] = spaced.reshape(groups, slots, lanes).astype(jnp.bfloat16)


def mixture_kernel(returned_ref, middle_ref, high_ref, low_ref, out_ref):
    groups, slots, lanes = returned_ref.shape
    returned = returned_ref[...].astype(jnp.float32).reshape(groups * slots, lanes)
    returned = returned.astype(jnp.bfloat16)
    mixture = sum(
        lax.dot_general(
            part[...], returned, (((0,), (0,)), ((), ())), preferred_element_type=jnp.float32
        )
        for part in (high_ref, low_ref)
    )
    out_ref[...] = (middle_ref[...] + mixture).astype(jnp.bfloat16)


def expert_kernel(rows_ref, gain_ref, *refs):
    both, out_ref = refs[:2], refs[2]
    blocks, rows, lanes = rows_ref.shape
    total = jnp.zeros((rows, lanes), jnp.float32)
    scaled = []
    for t in range(blocks):
        x = rows_ref[t].astype(jnp.float32)
        total = total + x * x
        scaled.append((x * gain_ref[t : t + 1, :]).astype(jnp.bfloat16))
    scaled = jnp.concatenate(scaled, axis=1)
    scale = lax.rsqrt(jnp.sum(total, axis=1, keepdims=True) / (blocks * lanes) + eps)
    width = blocks * lanes
    gate = jnp.concatenate([ref[:width] for ref in both], axis=1)
    gate = jnp.dot(scaled, gate, preferred_element_type=jnp.float32) * scale
    upper = jnp.concatenate([ref[width : 2 * width] for ref in both], axis=1)
    upper = jnp.dot(scaled, upper, preferred_element_type=jnp.float32) * scale
    gate = jnp.minimum(gate, limit)
    upper = jnp.clip(upper, -limit, limit)
    active = ((upper + 1.0) * gate * jax.nn.sigmoid(alpha * gate)).astype(jnp.bfloat16)
    columns = [
        jnp.concatenate([ref[start : start + lanes] for ref in both], axis=0)
        for start in range(2 * width, 3 * width, lanes)
    ]
    down = jnp.concatenate(columns, axis=1)
    result = jnp.dot(active, down, preferred_element_type=jnp.float32).astype(jnp.bfloat16)
    for t in range(blocks):
        out_ref[t] = result[:, t * lanes : (t + 1) * lanes]


def local(kernel, out_shape, *args, flops=0, far_in=0, far_out=0, scratch=()):
    def places(count, far):
        return [pl.BlockSpec(memory_space=pltpu.HBM)] * far + [
            pl.BlockSpec(memory_space=pltpu.VMEM)
        ] * (count - far)

    single = not isinstance(out_shape, list)
    outs = places(1 if single else len(out_shape), far_out)
    return pl.pallas_call(
        kernel,
        in_specs=places(len(args), far_in),
        out_specs=outs[0] if single else outs,
        out_shape=out_shape,
        scratch_shapes=scratch,
        compiler_params=pltpu.CompilerParams(vmem_limit_bytes=LIMIT),
        cost_estimate=pl.CostEstimate(flops=flops, bytes_accessed=0, transcendentals=0),
    )(*[pltpu.with_memory_space_constraint(x, pltpu.HBM) for x in args[:far_in]], *args[far_in:])


def exchange(x, axis):
    return lax.all_to_all(x, axis, 0, 0, tiled=True)


def layer(
    resid,
    attn_gain,
    w_query,
    w_key,
    w_value,
    key_cache,
    value_cache,
    key_bias,
    lengths,
    mix_gain,
    w_out,
    ffn_gain,
    route_experts,
    route_weights,
    w_gate,
    w_up,
    w_down,
):
    blocks = lax.axis_size(TP)
    groups = lax.axis_size(EP)
    rows, lanes = resid.shape
    heads = mix_gain.shape[0]
    items = groups * CAP
    bf16 = jnp.bfloat16
    shape = jax.ShapeDtypeStruct
    slots = groups * SLOTS
    new = shape((rows, heads), bf16)
    small = (
        resid,
        lengths.reshape(1, rows),
        attn_gain.reshape(blocks, lanes),
        mix_gain.reshape(1, heads),
        route_experts.T,
        route_weights.T,
    )
    near, *small = local(
        load_kernel,
        [shape(x.shape, x.dtype) for x in small],
        *small,
        far_in=len(small),
        scratch=[pltpu.SemaphoreType.DMA((len(small),))],
    )
    copies = local(copies_kernel, shape((blocks, rows, lanes), bf16), near, flops=LONG)
    new_keys, new_values, partial_branch, placed, high, low = local(
        attend_kernel,
        [new, new, shape((blocks, 2 * rows, lanes), bf16)] + [shape((slots, rows), bf16)] * 3,
        exchange(copies, TP),
        *small,
        w_query.T,
        w_key.T,
        w_value.T,
        key_cache,
        value_cache,
        key_bias,
        w_out,
        far_out=2,
        scratch=[pltpu.VMEM((2, rows, heads), bf16), pltpu.SemaphoreType.DMA((2,))],
    )
    pairs = [(i, i ^ PAIRS[i // blocks]) for i in range(CORES * blocks)]
    branch = exchange(partial_branch, TP)
    joined = local(
        join_kernel,
        shape((3 * blocks * lanes, lanes), bf16),
        w_gate,
        w_up,
        w_down,
        low,
        flops=SHORT,
    )
    swapped = lax.ppermute(joined, (EP[0], *TP), pairs)
    middle, outgoing = local(
        middle_kernel,
        [shape((rows, lanes), jnp.float32), shape((groups, SLOTS, lanes), bf16)],
        branch,
        near,
        placed,
        flops=SHORT,
    )
    held = local(
        spread_kernel, shape((blocks, items // 2, lanes), bf16), exchange(outgoing, EP), flops=SHORT
    )
    partial_out = local(
        expert_kernel,
        shape((blocks, items // 2, lanes), bf16),
        exchange(held, TP),
        ffn_gain.reshape(blocks, lanes),
        joined,
        swapped,
    )
    result = local(
        total_kernel, shape((groups, SLOTS, lanes), bf16), exchange(partial_out, TP), flops=SHORT
    )
    mixed = local(
        mixture_kernel, shape((rows, lanes), bf16), exchange(result, EP), middle, high, low
    )
    return (mixed, new_keys, new_values)


def solution(mesh):
    torus = Mesh(
        mesh.devices.reshape(mesh.shape["ep"] // CORES, CORES, 4, 4),
        ("ep_0", "ep_1", "tp_0", "tp_1"),
    )
    rows = ("ep_0", "ep_1")
    in_specs = (
        P(rows, TP),
        P(),
        P(None, TP),
        P(None, TP),
        P(None, TP),
        P(rows, TP, None, None),
        P(rows, TP, None, None),
        P(rows, TP, None),
        P(rows),
        P(TP),
        P(TP, None),
        P(),
        P(rows, None),
        P(rows, None),
        P(rows, None, TP),
        P(rows, None, TP),
        P(rows, TP, None),
    )
    out_specs = (P(rows, TP), P(rows, TP), P(rows, TP))
    return jax.shard_map(layer, mesh=torus, in_specs=in_specs, out_specs=out_specs, check_vma=False)
```
